128 devices in a mesh: dp: 4 (over x), kv: 16 (over z, y), tp: 2 (over core).
Axes of the slice: x: 4, y: 4, z: 4, core: 2. Of those that a mesh axis runs over, the one named last changes fastest.
Arguments:
- tokens: bfloat16 [512, 2048], P('dp', 'kv'), may hold values from -18 to 18
- mix_gain: float32 [2048], P('kv'), may hold values from 0.1 to 1.9
- w_query: bfloat16 [2048, 1024], P('kv', 'tp'), may hold values from -0.125 to 0.125
- w_key: bfloat16 [2048, 1024], P('kv', 'tp'), may hold values from -0.125 to 0.125
- w_value: bfloat16 [2048, 2048], P('kv', 'tp'), may hold values from -0.125 to 0.125
- w_outgate: bfloat16 [2048, 2048], P('kv', 'tp'), may hold values from -0.125 to 0.125
- w_gates: bfloat16 [2048, 16], replicated, may hold values from -0.25 to 0.25
- forget_bias: float32 [8], P('tp'), may hold values from -1 to 3
- memory: float32 [512, 8, 128, 256], P(('dp', 'kv'), 'tp'), may hold values from -4 to 4
- normalizer: float32 [512, 8, 128], P(('dp', 'kv'), 'tp'), may hold values from -4 to 4
- stabilizer: float32 [512, 8], P(('dp', 'kv'), 'tp'), may hold values from -4 to 4
- head_gain: float32 [8, 256], P('tp'), may hold values from 0.1 to 1.9
- w_out: bfloat16 [2048, 2048], P('tp', 'kv'), may hold values from -0.125 to 0.125
- mlp_gain: float32 [2048], replicated, may hold values from 0.1 to 1.9
- w_gate: bfloat16 [2048, 5632], P(None, ('kv', 'tp')), may hold values from -0.125 to 0.125
- w_up: bfloat16 [2048, 5632], P(None, ('kv', 'tp')), may hold values from -0.125 to 0.125
- w_down: bfloat16 [5632, 2048], P(('kv', 'tp')), may hold values from -0.15625 to 0.15625
Outputs:
- mixed_out: bfloat16 [512, 2048], P('dp', ('kv', 'tp'))
- new_memory: float32 [512, 8, 128, 256], P(('dp', 'kv'), 'tp')
- new_normalizer: float32 [512, 8, 128], P(('dp', 'kv'), 'tp')
- new_stabilizer: float32 [512, 8], P(('dp', 'kv'), 'tp')
The draws below stay inside these ranges and needn't reach their ends.
All inputs are finite; a program needn't handle non-finite values.
Results may differ from the reference program's by a relative error of at most 0.02.
Values may be sent and summed in bfloat16 or wider, within the bound.
No kernel may reach another device: no remote copies, remote signals or barrier semaphores. Data moves between devices by JAX's collectives and lax.ppermute only.
A program may use at most 64 MiB of HBM per device.

```python
import math
import jax
import jax.numpy as jnp
from jax import lax

D = 2048
HEADS = 8
QK = 128
VD = 256
FF = 5632
BATCH = 512
N_TP = 2


def draw_tokens(key, part):
    normal_key = jax.random.fold_in(jax.random.fold_in(key, 11), 0)
    columns = jnp.exp(jnp.linspace(0.0, math.log(3.0), D)).astype(jnp.float32)
    values_drawn = jnp.clip(jax.random.normal(normal_key, (BATCH, D), jnp.float32), -4.0, 4.0)
    return (values_drawn * columns).astype(jnp.bfloat16)


def strengthened(entries, stream_key, source, target, parts, factor):
    def block_of(dim):
        return (jnp.arange(entries.shape[dim]) // (entries.shape[dim] // parts)).reshape((-1,) + (1,) * (entries.ndim - 1 - dim))

    near = jax.random.permutation(stream_key, parts)[block_of(target)]
    far = (block_of(target) + parts // 2) % parts
    return jnp.where((block_of(source) == near) | (block_of(source) == far), factor * entries, entries)


def level_of(key, dims, cuts, least, largest):
    level, own = 1.0, jax.random.fold_in(key, 6)
    for axis_at, shards_of in cuts:
        heights = jnp.exp(jax.random.uniform(jax.random.fold_in(own, axis_at), (shards_of,), jnp.float32, least / len(cuts), largest / len(cuts)))
        level = level * jnp.repeat(heights, dims[axis_at] // shards_of).reshape([-1 if axis == axis_at else 1 for axis in range(len(dims))])
    return level


def centred(key, dims, width, bound, cuts=(), held_as=jnp.bfloat16):
    array = width * jax.random.normal(key, dims, jnp.float32)
    if cuts:
        array = array * level_of(key, dims, cuts, -0.22, 0.18)
    return jnp.clip(array, -bound, bound).astype(held_as)


def heavy_noise(stream_key, dims, scale, reach, shards, heavy, kind=jnp.bfloat16):
    values = scale * jax.random.normal(stream_key, dims, jnp.float32)
    if shards:
        values = values * level_of(stream_key, dims, shards, -0.22, 0.18)
    return jnp.clip(strengthened(values, jax.random.fold_in(stream_key, 3), *heavy), -reach, reach).astype(kind)


def setup_inputs(seed: int = 0) -> dict:
    arg_keys = jax.random.split(jax.random.key(seed), 18)
    tokens = draw_tokens(jax.random.fold_in(arg_keys[17], 71), 0)
    mix_gain = jnp.clip(1.0 + 0.18 * jax.random.normal(arg_keys[1], (D,), jnp.float32), 0.1, 1.9)
    w_query = centred(arg_keys[2], (D, HEADS * QK), D ** -0.5, 0.125, ((0, 16), (1, 2)))
    w_key = centred(arg_keys[3], (D, HEADS * QK), D ** -0.5, 0.125, ((0, 16), (1, 2)))
    w_value = centred(arg_keys[4], (D, HEADS * VD), D ** -0.5, 0.125, ((0, 16), (1, 2)))
    w_outgate = centred(arg_keys[5], (D, HEADS * VD), D ** -0.5, 0.125, ((0, 16), (1, 2)))
    w_gates = centred(arg_keys[6], (D, 2 * HEADS), (D // 4) ** -0.5, 0.25)
    forget_bias = jnp.clip(-1.0 + 4.0 * jax.random.uniform(arg_keys[7], (HEADS,), jnp.float32) ** level_of(arg_keys[7], (HEADS,), ((0, 2),), -0.2, 0.2), -1.0, 3.0)
    memory = centred(arg_keys[8], (BATCH, HEADS, QK, VD), 0.5, 4.0, ((0, 64), (1, 2)), jnp.float32)
    normalizer = centred(arg_keys[9], (BATCH, HEADS, QK), 0.5, 4.0, ((0, 64), (1, 2)), jnp.float32)
    stabilizer = centred(arg_keys[10], (BATCH, HEADS), 1.0, 4.0, ((0, 64), (1, 2)), jnp.float32)
    head_gain = jnp.clip(1.0 + 0.18 * jax.random.normal(arg_keys[11], (HEADS, VD), jnp.float32), 0.1, 1.9)
    w_out = centred(arg_keys[12], (HEADS * VD, D), (HEADS * VD) ** -0.5, 0.125, ((0, 2), (1, 16)))
    mlp_gain = jnp.clip(1.0 + 0.18 * jax.random.normal(arg_keys[13], (D,), jnp.float32), 0.1, 1.9)
    w_gate = centred(arg_keys[14], (D, FF), D ** -0.5, 0.125, ((1, 32),))
    w_up = centred(arg_keys[15], (D, FF), D ** -0.5, 0.125, ((1, 32),))
    w_down = heavy_noise(arg_keys[16], (FF, D), FF ** -0.5, 0.15625, ((0, 32),), (0, 1, 32, 2.75))
    return {"tokens": tokens, "mix_gain": mix_gain, "w_query": w_query, "w_key": w_key, "w_value": w_value, "w_outgate": w_outgate, "w_gates": w_gates, "forget_bias": forget_bias, "memory": memory, "normalizer": normalizer, "stabilizer": stabilizer, "head_gain": head_gain, "w_out": w_out, "mlp_gain": mlp_gain, "w_gate": w_gate, "w_up": w_up, "w_down": w_down}


EPSILON = 1e-06

def reference(tokens, mix_gain, w_query, w_key, w_value, w_outgate, w_gates, forget_bias, memory, normalizer, stabilizer, head_gain, w_out, mlp_gain, w_gate, w_up, w_down):
    activations = tokens.astype(jnp.float32)
    batch_rows = tokens.shape[0]
    inverse = lax.rsqrt(lax.optimization_barrier(jnp.mean(activations * activations, axis=1, keepdims=True)) + EPSILON)
    scaled = (activations * mix_gain).astype(jnp.bfloat16)
    query_rows = (jnp.dot(scaled, w_query, preferred_element_type=jnp.float32) * inverse).astype(jnp.bfloat16)
    key_rows = (jnp.dot(scaled, w_key, preferred_element_type=jnp.float32) * (inverse * QK ** (-0.5))).astype(jnp.bfloat16)
    value_rows = (jnp.dot(scaled, w_value, preferred_element_type=jnp.float32) * inverse).astype(jnp.bfloat16)
    outgate = (jnp.dot(scaled, w_outgate, preferred_element_type=jnp.float32) * inverse).astype(jnp.bfloat16)
    gate_pre = jnp.dot(scaled, w_gates, preferred_element_type=jnp.float32) * inverse
    input_pre = gate_pre[:, :HEADS]
    log_forget = jax.nn.log_sigmoid(gate_pre[:, HEADS:] + forget_bias)
    new_stabilizer = jnp.maximum(log_forget + stabilizer, input_pre)
    forget_scale = jnp.exp(log_forget + stabilizer - new_stabilizer)
    input_scale = jnp.exp(input_pre - new_stabilizer)
    query_heads = query_rows.astype(jnp.float32).reshape(batch_rows, HEADS, QK)
    key_heads = key_rows.astype(jnp.float32).reshape(batch_rows, HEADS, QK)
    value_heads = value_rows.astype(jnp.float32).reshape(batch_rows, HEADS, VD)
    new_normalizer = forget_scale[..., None] * normalizer + input_scale[..., None] * key_heads
    denominator = lax.optimization_barrier(jnp.sum(query_heads * new_normalizer, axis=2))
    carried = jnp.einsum('bhd,bhde->bhe', query_heads, memory, precision=lax.Precision.HIGHEST)
    query_key = lax.optimization_barrier(jnp.sum(query_heads * key_heads, axis=2))
    numerator = forget_scale[..., None] * carried + (input_scale * query_key)[..., None] * value_heads
    new_memory = forget_scale[..., None, None] * memory + (input_scale[..., None] * key_heads)[..., None] * value_heads[:, :, None, :]
    head_out = numerator / jnp.maximum(jnp.abs(denominator), 1.0)[..., None]
    normed = head_out * lax.rsqrt(lax.optimization_barrier(jnp.mean(head_out * head_out, axis=2, keepdims=True)) + EPSILON) * head_gain
    mixed_heads = (normed.reshape(batch_rows, HEADS * VD) * jax.nn.sigmoid(outgate.astype(jnp.float32))).astype(jnp.bfloat16)
    group_width = HEADS * VD // N_TP
    branch = jnp.zeros((batch_rows, D), jnp.float32)
    for group in range(N_TP):
        partial_out = jnp.dot(mixed_heads[:, group * group_width:(group + 1) * group_width], w_out[group * group_width:(group + 1) * group_width], preferred_element_type=jnp.float32).astype(jnp.bfloat16)
        branch = branch + lax.optimization_barrier(partial_out).astype(jnp.float32)
    residual = (activations + branch).astype(jnp.bfloat16)
    resid_float = residual.astype(jnp.float32)
    inverse_two = lax.rsqrt(lax.optimization_barrier(jnp.mean(resid_float * resid_float, axis=1, keepdims=True)) + EPSILON)
    mlp_in = (resid_float * inverse_two * mlp_gain).astype(jnp.bfloat16)
    gate_value = jnp.dot(mlp_in, w_gate, preferred_element_type=jnp.float32)
    up_value = jnp.dot(mlp_in, w_up, preferred_element_type=jnp.float32)
    hidden = (jax.nn.silu(gate_value) * up_value).astype(jnp.bfloat16)
    mixed_out = (jnp.dot(hidden, w_down, preferred_element_type=jnp.float32) + resid_float).astype(jnp.bfloat16)
    return (mixed_out, new_memory, new_normalizer, new_stabilizer)
```

```python
import jax
import jax.numpy as jnp
from jax import lax
from jax.experimental import pallas as pl
from jax.experimental.pallas import tpu as pltpu
from jax.sharding import PartitionSpec as P

QK = 128
VD = 256
EPSILON = 1e-06
LANES = 128
F32 = jnp.float32
BF16 = jnp.bfloat16
NT = (((1,), (1,)), ((), ()))
VMEM = pltpu.MemorySpace.VMEM
SMEM = pltpu.MemorySpace.SMEM
HBM = pltpu.MemorySpace.HBM


def spec(space):
    return pl.BlockSpec(memory_space=space)


def project_kernel(tokens, gain, wq, wk, wv, wo, wg, out, bq, bk, bv, bo, bg, sems):
    copies = []
    cols = tokens.shape[1]
    kv = lax.axis_index("kv")
    gate_src = wg.at[:, pl.ds(pl.multiple_of(kv * cols, LANES), cols)]
    for n, (src, dst) in enumerate(((wq, bq), (wk, bk), (gate_src, bg), (wv, bv), (wo, bo))):
        copy = pltpu.make_async_copy(src, dst, sems.at[n])
        copy.start()
        copies.append(copy)
    blocks, rows = out.shape[:2]
    act = tokens[...].astype(F32)
    square = jnp.sum(act * act, axis=1, keepdims=True)
    scaled = (act * gain[...]).astype(BF16)

    def put(value, at):
        width = value.shape[1]
        out[:, :, at : at + width] = value.reshape(blocks, rows, width).astype(BF16)

    at = 0
    for n, buf in ((0, bq), (1, bk)):
        copies[n].wait()
        put(jnp.dot(scaled, buf[...], preferred_element_type=F32), at)
        at += buf.shape[1]
    copies[2].wait()
    gate_count = bg.shape[0]
    wide = jnp.concatenate([bg[...].astype(F32), jnp.zeros((LANES - gate_count, cols), F32)], axis=0)
    gates = lax.dot_general(scaled, wide.astype(BF16), NT, preferred_element_type=F32)
    lane = lax.broadcasted_iota(jnp.int32, gates.shape, 1)
    gates = jnp.where(lane == gate_count, square, gates)
    for n, buf in ((3, bv), (4, bo)):
        copies[n].wait()
        put(jnp.dot(scaled, buf[...], preferred_element_type=F32), at)
        at += buf.shape[1]
    put(gates, at)


def project(tokens, mix_gain, w_query, w_key, w_value, w_outgate, w_gates, blocks):
    rows, cols = tokens.shape
    width = w_query.shape[1] + w_key.shape[1] + w_value.shape[1] + w_outgate.shape[1] + LANES
    weights = (w_query, w_key, w_value, w_outgate)
    return pl.pallas_call(
        project_kernel,
        out_shape=jax.ShapeDtypeStruct((blocks, rows // blocks, width), BF16),
        in_specs=[spec(VMEM)] * 2 + [spec(HBM)] * 5,
        out_specs=spec(VMEM),
        scratch_shapes=[pltpu.VMEM(w.shape, BF16) for w in weights]
        + [pltpu.VMEM((w_gates.shape[1], cols), BF16), pltpu.SemaphoreType.DMA((5,))],
        name="project",
    )(tokens, mix_gain[None], *weights, w_gates.T)


def state_kernel(
    recv, bias, memory, normalizer, stab, gain,
    heads, norm_out, stab_out, forget_out, key_out, value_out,
    mem, sems, *, model_width, total_heads,
):
    seqs, local = memory.shape[0], memory.shape[1]
    copies = []
    for h in range(local):
        copy = pltpu.make_async_copy(memory.at[:, h], mem.at[h], sems.at[h])
        copy.start()
        copies.append(copy)
    tp = lax.axis_index("tp")
    qw, vw = local * QK, local * VD

    def summed(lo, width):
        return jnp.sum(recv[:, :, lo : lo + width].astype(F32), axis=0)

    small = summed(2 * qw + 2 * vw, LANES)
    inverse = lax.rsqrt(small[:, 2 * total_heads : 2 * total_heads + 1] / model_width + EPSILON)
    query = (summed(0, qw) * inverse).astype(BF16).astype(F32)
    key = (summed(qw, qw) * (inverse * QK ** (-0.5))).astype(BF16).astype(F32)
    value = (summed(2 * qw, vw) * inverse).astype(BF16).astype(F32)
    outgate = (summed(2 * qw + vw, vw) * inverse).astype(BF16).astype(F32)
    row = lax.broadcasted_iota(jnp.int32, (seqs, QK), 0)
    diag = lax.broadcasted_iota(jnp.int32, (seqs, seqs), 0) == lax.broadcasted_iota(
        jnp.int32, (seqs, seqs), 1
    )

    def own(at, h):
        both = [small[:, at + t * local + h : at + t * local + h + 1] for t in range(total_heads // local)]
        got = both[0]
        for t in range(1, len(both)):
            got = jnp.where(tp == t, both[t], got)
        return got

    partial = []
    for h in range(local):
        input_pre = own(0, h) * inverse
        log_forget = jax.nn.log_sigmoid(own(total_heads, h) * inverse + bias[h])
        old = jnp.sum(jnp.where(diag, stab[h : h + 1, :], 0.0), axis=1, keepdims=True)
        new = jnp.maximum(log_forget + old, input_pre)
        forget = jnp.exp(log_forget + old - new)
        scale = jnp.exp(input_pre - new)
        stab_out[h : h + 1, :] = jnp.sum(jnp.where(diag, new, 0.0), axis=0, keepdims=True)
        q, k = query[:, h * QK : (h + 1) * QK], key[:, h * QK : (h + 1) * QK]
        scaled_key = scale * k
        new_norm = forget * normalizer[:, h, :] + scaled_key
        norm_out[:, h, :] = new_norm
        key_out[:, h, :] = scaled_key
        v = value[:, h * VD : (h + 1) * VD]
        value_out[:, h, :] = v
        forget_out[:, h, :] = jnp.broadcast_to(forget, (seqs, LANES))
        denom = jnp.maximum(jnp.abs(jnp.sum(q * new_norm, axis=1, keepdims=True)), 1.0)
        query_key = jnp.sum(q * k, axis=1, keepdims=True)
        spread = [jnp.where(row == b, q, 0.0).astype(BF16) for b in range(seqs)]
        partial.append((forget, (scale * query_key) * v, denom, spread))
    for h in range(local):
        forget, fresh, denom, spread = partial[h]
        copies[h].wait()
        carried = jnp.zeros((seqs, VD), F32)
        for b in range(0, seqs, 2):
            left = jnp.concatenate([spread[b], spread[b + 1]], axis=1)
            right = mem[h, b : b + 2].reshape(2 * QK, VD).astype(BF16)
            carried = carried + jnp.dot(left, right, preferred_element_type=F32)
        head_out = (forget * carried + fresh) / denom
        normed = head_out * lax.rsqrt(jnp.mean(head_out * head_out, axis=1, keepdims=True) + EPSILON)
        gate = jax.nn.sigmoid(outgate[:, h * VD : (h + 1) * VD])
        mixed = (normed * gain[h : h + 1, :] * gate).astype(BF16)
        heads[:, :, h * VD : (h + 1) * VD] = jnp.broadcast_to(mixed[None], (heads.shape[0], seqs, VD))


def state_step(recv, forget_bias, memory, normalizer, stabilizer, head_gain, model_width, total_heads):
    blocks = recv.shape[0]
    seqs, local = memory.shape[:2]

    def kernel(*refs):
        state_kernel(*refs, model_width=model_width, total_heads=total_heads)

    return pl.pallas_call(
        kernel,
        out_shape=(
            jax.ShapeDtypeStruct((blocks, seqs, local * VD), BF16),
            jax.ShapeDtypeStruct((seqs, local, QK), F32),
            jax.ShapeDtypeStruct((local, seqs), F32),
            jax.ShapeDtypeStruct((seqs, local, LANES), F32),
            jax.ShapeDtypeStruct((seqs, local, QK), F32),
            jax.ShapeDtypeStruct((seqs, local, VD), F32),
        ),
        in_specs=[spec(VMEM), spec(SMEM), spec(HBM), spec(VMEM), spec(VMEM), spec(VMEM)],
        out_specs=[spec(VMEM)] * 6,
        scratch_shapes=[
            pltpu.VMEM((local, seqs, QK, VD), F32),
            pltpu.SemaphoreType.DMA((local,)),
        ],
        name="state",
    )(recv, forget_bias, memory, normalizer, stabilizer.T, head_gain)


def mixer_kernel(rows_ref, gain, wg, wu, wd, keep, give, mlp):
    blocks, rows, cols = rows_ref.shape
    tp = lax.axis_index("tp")
    total = jnp.zeros((rows, cols), F32)
    for j in range(blocks):
        value = rows_ref[j].astype(F32)
        total = total + value * value
    inverse = lax.rsqrt(jnp.sum(total, axis=1, keepdims=True) / (blocks * cols) + EPSILON)
    for j in range(blocks):
        lo = j * cols
        value = rows_ref[j].astype(F32) * inverse * gain[:, lo : lo + cols]
        mlp[:, lo : lo + cols] = value.astype(BF16)
    gate = lax.dot_general(mlp[...], wg[...], NT, preferred_element_type=F32)
    up = lax.dot_general(mlp[...], wu[...], NT, preferred_element_type=F32)
    hidden = (jax.nn.silu(gate) * up).astype(BF16)
    half = keep.shape[1]
    for j in range(blocks):
        part = jnp.dot(hidden, wd[:, j * cols : (j + 1) * cols], preferred_element_type=F32).T
        first, second = part[:half].astype(BF16), part[half:].astype(BF16)
        keep[j] = jnp.where(tp == 0, first, second)
        give[j] = jnp.where(tp == 0, second, first)


def mixer(gathered, mlp_gain, w_gate, w_up, w_down):
    blocks, rows, cols = gathered.shape
    half = jax.ShapeDtypeStruct((blocks, cols // 2, rows), BF16)
    return pl.pallas_call(
        mixer_kernel,
        out_shape=(half, half),
        in_specs=[spec(VMEM)] * 5,
        out_specs=[spec(VMEM)] * 2,
        scratch_shapes=[pltpu.VMEM((rows, blocks * cols), BF16)],
        name="mixer",
    )(gathered, mlp_gain[None], w_gate.T, w_up.T, w_down)


def other_core(value):
    return lax.ppermute(value, "tp", [(0, 1), (1, 0)])


def exchanged(blocks):
    return lax.all_to_all(blocks, "kv", 0, 0, tiled=True)


def body(
    tokens,
    mix_gain,
    w_query,
    w_key,
    w_value,
    w_outgate,
    w_gates,
    forget_bias,
    memory,
    normalizer,
    stabilizer,
    head_gain,
    w_out,
    mlp_gain,
    w_gate,
    w_up,
    w_down,
):
    devices = lax.axis_size("kv")
    rows, block_cols = tokens.shape
    send = project(tokens, mix_gain, w_query, w_key, w_value, w_outgate, w_gates, devices)
    heads, new_normalizer, new_stabilizer, forget, scaled_key, value = state_step(
        exchanged(send),
        forget_bias,
        memory,
        normalizer,
        stabilizer,
        head_gain,
        block_cols * devices,
        w_gates.shape[1] // 2,
    )
    gathered_heads = exchanged(heads).reshape(rows, -1)
    branch = jnp.dot(gathered_heads, w_out, preferred_element_type=F32).astype(BF16)
    residual = (
        tokens.astype(F32) + (branch.astype(F32) + other_core(branch).astype(F32))
    ).astype(BF16)
    gathered = exchanged(jnp.broadcast_to(residual[None], (devices, *residual.shape)))
    keep, give = mixer(gathered, mlp_gain, w_gate, w_up, w_down)
    pair = (keep.astype(F32) + other_core(give).astype(F32)).astype(BF16)
    late_forget, late_key, late_value, _ = lax.optimization_barrier((forget, scaled_key, value, keep))
    new_memory = (
        late_forget[:, :, :1, None] * memory + late_key[..., None] * late_value[:, :, None, :]
    )
    summed = jnp.sum(exchanged(pair).astype(F32), axis=0)
    out_cols = block_cols // lax.axis_size("tp")
    own = lax.dynamic_slice_in_dim(residual, lax.axis_index("tp") * out_cols, out_cols, 1)
    mixed_out = (summed + own.T.astype(F32)).astype(BF16).T
    return (mixed_out, new_memory, new_normalizer, new_stabilizer.T)


def solution(mesh):
    in_specs = (
        P("dp", "kv"),
        P("kv"),
        P("kv", "tp"),
        P("kv", "tp"),
        P("kv", "tp"),
        P("kv", "tp"),
        P(),
        P("tp"),
        P(("dp", "kv"), "tp", None, None),
        P(("dp", "kv"), "tp", None),
        P(("dp", "kv"), "tp"),
        P("tp", None),
        P("tp", "kv"),
        P(),
        P(None, ("kv", "tp")),
        P(None, ("kv", "tp")),
        P(("kv", "tp"), None),
    )
    out_specs = (
        P("dp", ("kv", "tp")),
        P(("dp", "kv"), "tp", None, None),
        P(("dp", "kv"), "tp", None),
        P(("dp", "kv"), "tp"),
    )
    return jax.shard_map(body, mesh=mesh, in_specs=in_specs, out_specs=out_specs, check_vma=False)
```

```python
import jax
import jax.numpy as jnp
from jax import lax
from jax.experimental import pallas as pl
from jax.experimental.pallas import tpu as pltpu
from jax.sharding import PartitionSpec as P

QK = 128
VD = 256
EPSILON = 1e-06
LANES = 128
F32 = jnp.float32
BF16 = jnp.bfloat16
NT = (((1,), (1,)), ((), ()))
VMEM = pltpu.MemorySpace.VMEM
SMEM = pltpu.MemorySpace.SMEM
HBM = pltpu.MemorySpace.HBM


def spec(space):
    return pl.BlockSpec(memory_space=space)


def stay(*arrays):
    return [pltpu.with_memory_space_constraint(a, HBM) for a in arrays]


def fetch(pairs, sems):
    copies = [pltpu.make_async_copy(src, dst, sems.at[n]) for n, (src, dst) in enumerate(pairs)]
    for copy in copies:
        copy.start()
    return copies


def project_kernel(tokens, gain, wq, wk, wv, wo, wg, out, bt, bn, bq, bk, bv, bo, bg, sems):
    cols = tokens.shape[1]
    kv = lax.axis_index("kv")
    gate_src = wg.at[:, pl.ds(pl.multiple_of(kv * cols, LANES), cols)]
    copies = fetch(
        ((tokens, bt), (gain, bn), (wq, bq), (wk, bk), (gate_src, bg), (wv, bv), (wo, bo)), sems
    )
    blocks, rows = out.shape[:2]
    copies[0].wait()
    copies[1].wait()
    act = bt[...].astype(F32)
    square = jnp.sum(act * act, axis=1, keepdims=True)
    scaled = (act * bn[...]).astype(BF16)

    def put(value, at):
        width = value.shape[1]
        out[:, :, at : at + width] = value.reshape(blocks, rows, width).astype(BF16)

    at = 0
    for n, buf in ((2, bq), (3, bk), (5, bv), (6, bo)):
        copies[n].wait()
        put(jnp.dot(scaled, buf[...], preferred_element_type=F32), at)
        at += buf.shape[1]
    copies[4].wait()
    gate_count = bg.shape[0]
    wide = jnp.concatenate([bg[...].astype(F32), jnp.zeros((LANES - gate_count, cols), F32)], axis=0)
    gates = lax.dot_general(scaled, wide.astype(BF16), NT, preferred_element_type=F32)
    lane = lax.broadcasted_iota(jnp.int32, gates.shape, 1)
    put(jnp.where(lane == gate_count, square, gates), at)


def project(tokens, mix_gain, w_query, w_key, w_value, w_outgate, w_gates, blocks):
    rows, cols = tokens.shape
    width = w_query.shape[1] + w_key.shape[1] + w_value.shape[1] + w_outgate.shape[1] + LANES
    weights = (w_query, w_key, w_value, w_outgate)
    return pl.pallas_call(
        project_kernel,
        out_shape=jax.ShapeDtypeStruct((blocks, rows // blocks, width), BF16),
        in_specs=[spec(HBM)] * 7,
        out_specs=spec(VMEM),
        scratch_shapes=[pltpu.VMEM((rows, cols), BF16), pltpu.VMEM((1, cols), F32)]
        + [pltpu.VMEM(w.shape, BF16) for w in weights]
        + [pltpu.VMEM((w_gates.shape[1], cols), BF16), pltpu.SemaphoreType.DMA((7,))],
        compiler_params=pltpu.CompilerParams(vmem_limit_bytes=8 << 20),
        name="project",
    )(*stay(tokens, mix_gain[None], *weights, w_gates.T))


def state_kernel(
    recv, bias_src, memory, norm_src, stab_src, gain_src,
    heads, norm_out, stab_out, forget_out, key_out, value_out,
    bias, normalizer, stab, gain, mem, sems, *, model_width, total_heads,
):
    seqs, local = memory.shape[0], memory.shape[1]
    copies = fetch(
        ((bias_src, bias), (norm_src, normalizer), (stab_src, stab), (gain_src, gain))
        + tuple((memory.at[:, h], mem.at[h]) for h in range(local)),
        sems,
    )
    tp = lax.axis_index("tp")
    qw, vw = local * QK, local * VD

    def summed(lo, width):
        return jnp.sum(recv[:, :, lo : lo + width].astype(F32), axis=0)

    small = summed(2 * qw + 2 * vw, LANES)
    inverse = lax.rsqrt(small[:, 2 * total_heads : 2 * total_heads + 1] / model_width + EPSILON)
    query = (summed(0, qw) * inverse).astype(BF16).astype(F32)
    key = (summed(qw, qw) * (inverse * QK ** (-0.5))).astype(BF16).astype(F32)
    value = (summed(2 * qw, vw) * inverse).astype(BF16).astype(F32)
    outgate = (summed(2 * qw + vw, vw) * inverse).astype(BF16).astype(F32)
    row = lax.broadcasted_iota(jnp.int32, (seqs, QK), 0)
    diag = lax.broadcasted_iota(jnp.int32, (seqs, seqs), 0) == lax.broadcasted_iota(
        jnp.int32, (seqs, seqs), 1
    )
    for copy in copies[:4]:
        copy.wait()

    def own(at, h):
        both = [small[:, at + t * local + h : at + t * local + h + 1] for t in range(total_heads // local)]
        got = both[0]
        for t in range(1, len(both)):
            got = jnp.where(tp == t, both[t], got)
        return got

    partial = []
    for h in range(local):
        input_pre = own(0, h) * inverse
        log_forget = jax.nn.log_sigmoid(own(total_heads, h) * inverse + bias[:, h : h + 1])
        old = jnp.sum(jnp.where(diag, stab[h : h + 1, :], 0.0), axis=1, keepdims=True)
        new = jnp.maximum(log_forget + old, input_pre)
        forget = jnp.exp(log_forget + old - new)
        scale = jnp.exp(input_pre - new)
        stab_out[h : h + 1, :] = jnp.sum(jnp.where(diag, new, 0.0), axis=0, keepdims=True)
        q, k = query[:, h * QK : (h + 1) * QK], key[:, h * QK : (h + 1) * QK]
        scaled_key = scale * k
        new_norm = forget * normalizer[:, h, :] + scaled_key
        norm_out[:, h, :] = new_norm
        key_out[:, h, :] = scaled_key
        v = value[:, h * VD : (h + 1) * VD]
        value_out[:, h, :] = v
        forget_out[:, h, :] = jnp.broadcast_to(forget, (seqs, LANES))
        denom = jnp.maximum(jnp.abs(jnp.sum(q * new_norm, axis=1, keepdims=True)), 1.0)
        query_key = jnp.sum(q * k, axis=1, keepdims=True)
        spread = [jnp.where(row == b, q, 0.0).astype(BF16) for b in range(seqs)]
        partial.append((forget, (scale * query_key) * v, denom, spread))
    for h in range(local):
        forget, fresh, denom, spread = partial[h]
        copies[4 + h].wait()
        carried = jnp.zeros((seqs, VD), F32)
        for b in range(0, seqs, 2):
            left = jnp.concatenate([spread[b], spread[b + 1]], axis=1)
            right = mem[h, b : b + 2].reshape(2 * QK, VD).astype(BF16)
            carried = carried + jnp.dot(left, right, preferred_element_type=F32)
        head_out = (forget * carried + fresh) / denom
        normed = head_out * lax.rsqrt(jnp.mean(head_out * head_out, axis=1, keepdims=True) + EPSILON)
        gate = jax.nn.sigmoid(outgate[:, h * VD : (h + 1) * VD])
        mixed = (normed * gain[h : h + 1, :] * gate).astype(BF16)
        heads[:, :, h * VD : (h + 1) * VD] = jnp.broadcast_to(mixed[None], (heads.shape[0], seqs, VD))


def state_step(recv, forget_bias, memory, normalizer, stabilizer, head_gain, model_width, total_heads):
    blocks = recv.shape[0]
    seqs, local = memory.shape[:2]

    def kernel(*refs):
        state_kernel(*refs, model_width=model_width, total_heads=total_heads)

    return pl.pallas_call(
        kernel,
        out_shape=(
            jax.ShapeDtypeStruct((blocks, seqs, local * VD), BF16),
            jax.ShapeDtypeStruct((seqs, local, QK), F32),
            jax.ShapeDtypeStruct((local, seqs), F32),
            jax.ShapeDtypeStruct((seqs, local, LANES), F32),
            jax.ShapeDtypeStruct((seqs, local, QK), F32),
            jax.ShapeDtypeStruct((seqs, local, VD), F32),
        ),
        in_specs=[spec(VMEM)] + [spec(HBM)] * 5,
        out_specs=[spec(VMEM)] * 6,
        scratch_shapes=[
            pltpu.VMEM((1, local), F32),
            pltpu.VMEM((seqs, local, QK), F32),
            pltpu.VMEM((local, seqs), F32),
            pltpu.VMEM((local, VD), F32),
            pltpu.VMEM((local, seqs, QK, VD), F32),
            pltpu.SemaphoreType.DMA((4 + local,)),
        ],
        compiler_params=pltpu.CompilerParams(vmem_limit_bytes=16 << 20),
        name="state",
    )(recv, *stay(forget_bias[None], memory, normalizer, stabilizer.T, head_gain))


def mixer_kernel(rows_ref, gain, wg, wu, wd, keep, give, mlp):
    blocks, rows, cols = rows_ref.shape
    tp = lax.axis_index("tp")
    total = jnp.zeros((rows, cols), F32)
    for j in range(blocks):
        value = rows_ref[j].astype(F32)
        total = total + value * value
    inverse = lax.rsqrt(jnp.sum(total, axis=1, keepdims=True) / (blocks * cols) + EPSILON)
    for j in range(blocks):
        lo = j * cols
        value = rows_ref[j].astype(F32) * inverse * gain[:, lo : lo + cols]
        mlp[:, lo : lo + cols] = value.astype(BF16)
    gate = lax.dot_general(mlp[...], wg[...], NT, preferred_element_type=F32)
    up = lax.dot_general(mlp[...], wu[...], NT, preferred_element_type=F32)
    hidden = (jax.nn.silu(gate) * up).astype(BF16)
    half = keep.shape[1]
    for j in range(blocks):
        part = jnp.dot(hidden, wd[:, j * cols : (j + 1) * cols], preferred_element_type=F32).T
        first, second = part[:half].astype(BF16), part[half:].astype(BF16)
        keep[j] = jnp.where(tp == 0, first, second)
        give[j] = jnp.where(tp == 0, second, first)


def mixer(gathered, mlp_gain, w_gate, w_up, w_down):
    blocks, rows, cols = gathered.shape
    half = jax.ShapeDtypeStruct((blocks, cols // 2, rows), BF16)
    return pl.pallas_call(
        mixer_kernel,
        out_shape=(half, half),
        in_specs=[spec(VMEM)] * 5,
        out_specs=[spec(VMEM)] * 2,
        scratch_shapes=[pltpu.VMEM((rows, blocks * cols), BF16)],
        compiler_params=pltpu.CompilerParams(vmem_limit_bytes=16 << 20),
        name="mixer",
    )(gathered, mlp_gain[None], w_gate.T, w_up.T, w_down)


def other_core(value):
    return lax.ppermute(value, "tp", [(0, 1), (1, 0)])


def exchanged(blocks):
    return lax.all_to_all(blocks, "kv", 0, 0, tiled=True)


def body(
    tokens,
    mix_gain,
    w_query,
    w_key,
    w_value,
    w_outgate,
    w_gates,
    forget_bias,
    memory,
    normalizer,
    stabilizer,
    head_gain,
    w_out,
    mlp_gain,
    w_gate,
    w_up,
    w_down,
):
    devices = lax.axis_size("kv")
    rows, block_cols = tokens.shape
    send = project(tokens, mix_gain, w_query, w_key, w_value, w_outgate, w_gates, devices)
    heads, new_normalizer, new_stabilizer, forget, scaled_key, value = state_step(
        exchanged(send),
        forget_bias,
        memory,
        normalizer,
        stabilizer,
        head_gain,
        block_cols * devices,
        w_gates.shape[1] // 2,
    )
    gathered_heads = exchanged(heads).reshape(rows, -1)
    branch = jnp.dot(gathered_heads, w_out, preferred_element_type=F32).astype(BF16)
    residual = (
        tokens.astype(F32) + (branch.astype(F32) + other_core(branch).astype(F32))
    ).astype(BF16)
    gathered = exchanged(jnp.broadcast_to(residual[None], (devices, *residual.shape)))
    keep, give = mixer(gathered, mlp_gain, w_gate, w_up, w_down)
    pair = (keep.astype(F32) + other_core(give).astype(F32)).astype(BF16)
    late_forget, late_key, late_value, _ = lax.optimization_barrier((forget, scaled_key, value, keep))
    new_memory = (
        late_forget[:, :, :1, None] * memory + late_key[..., None] * late_value[:, :, None, :]
    )
    summed = jnp.sum(exchanged(pair).astype(F32), axis=0)
    out_cols = block_cols // lax.axis_size("tp")
    own = lax.dynamic_slice_in_dim(residual, lax.axis_index("tp") * out_cols, out_cols, 1)
    mixed_out = (summed + own.T.astype(F32)).astype(BF16).T
    return (mixed_out, new_memory, new_normalizer, new_stabilizer.T)


def solution(mesh):
    in_specs = (
        P("dp", "kv"),
        P("kv"),
        P("kv", "tp"),
        P("kv", "tp"),
        P("kv", "tp"),
        P("kv", "tp"),
        P(),
        P("tp"),
        P(("dp", "kv"), "tp", None, None),
        P(("dp", "kv"), "tp", None),
        P(("dp", "kv"), "tp"),
        P("tp", None),
        P("tp", "kv"),
        P(),
        P(None, ("kv", "tp")),
        P(None, ("kv", "tp")),
        P(("kv", "tp"), None),
    )
    out_specs = (
        P("dp", ("kv", "tp")),
        P(("dp", "kv"), "tp", None, None),
        P(("dp", "kv"), "tp", None),
        P(("dp", "kv"), "tp"),
    )
    return jax.shard_map(body, mesh=mesh, in_specs=in_specs, out_specs=out_specs, check_vma=False)
```

```python
import jax
import jax.numpy as jnp
from jax import lax
from jax.experimental import pallas as pl
from jax.experimental.pallas import tpu as pltpu
from jax.sharding import PartitionSpec as P

QK = 128
VD = 256
EPSILON = 1e-06
LANES = 128
F32 = jnp.float32
BF16 = jnp.bfloat16
NT = (((1,), (1,)), ((), ()))
VMEM = pltpu.MemorySpace.VMEM
SMEM = pltpu.MemorySpace.SMEM
HBM = pltpu.MemorySpace.HBM


def spec(space):
    return pl.BlockSpec(memory_space=space)


def stay(*arrays):
    return [pltpu.with_memory_space_constraint(a, HBM) for a in arrays]


def fetch(pairs, sems):
    copies = [pltpu.make_async_copy(src, dst, sems.at[n]) for n, (src, dst) in enumerate(pairs)]
    for copy in copies:
        copy.start()
    return copies


def project_kernel(tokens, gain, wq, wk, wv, wo, wg, out, bt, bn, bq, bk, bv, bo, bg, sems):
    cols = tokens.shape[1]
    kv = lax.axis_index("kv")
    gate_src = wg.at[:, pl.ds(pl.multiple_of(kv * cols, LANES), cols)]
    copies = fetch(
        ((tokens, bt), (gain, bn), (wq, bq), (wk, bk), (gate_src, bg), (wv, bv), (wo, bo)), sems
    )
    blocks, rows = out.shape[:2]
    copies[0].wait()
    copies[1].wait()
    act = bt[...].astype(F32)
    square = jnp.sum(act * act, axis=1, keepdims=True)
    scaled = (act * bn[...]).astype(BF16)

    def put(value, at):
        width = value.shape[1]
        out[:, :, at : at + width] = value.reshape(blocks, rows, width).astype(BF16)

    at = 0
    for n, buf in ((2, bq), (3, bk), (5, bv), (6, bo)):
        copies[n].wait()
        put(jnp.dot(scaled, buf[...], preferred_element_type=F32), at)
        at += buf.shape[1]
    copies[4].wait()
    gate_count = bg.shape[0]
    wide = jnp.concatenate([bg[...].astype(F32), jnp.zeros((LANES - gate_count, cols), F32)], axis=0)
    gates = lax.dot_general(scaled, wide.astype(BF16), NT, preferred_element_type=F32)
    lane = lax.broadcasted_iota(jnp.int32, gates.shape, 1)
    put(jnp.where(lane == gate_count, square, gates), at)


def project(tokens, mix_gain, w_query, w_key, w_value, w_outgate, w_gates, blocks):
    rows, cols = tokens.shape
    width = w_query.shape[1] + w_key.shape[1] + w_value.shape[1] + w_outgate.shape[1] + LANES
    weights = (w_query, w_key, w_value, w_outgate)
    return pl.pallas_call(
        project_kernel,
        out_shape=jax.ShapeDtypeStruct((blocks, rows // blocks, width), BF16),
        in_specs=[spec(HBM)] * 7,
        out_specs=spec(VMEM),
        scratch_shapes=[pltpu.VMEM((rows, cols), BF16), pltpu.VMEM((1, cols), F32)]
        + [pltpu.VMEM(w.shape, BF16) for w in weights]
        + [pltpu.VMEM((w_gates.shape[1], cols), BF16), pltpu.SemaphoreType.DMA((7,))],
        compiler_params=pltpu.CompilerParams(vmem_limit_bytes=8 << 20),
        cost_estimate=pl.CostEstimate(flops=10**10, bytes_accessed=10**7, transcendentals=0),
        name="project",
    )(*stay(tokens, mix_gain[None], *weights, w_gates.T))


def state_kernel(
    recv, bias, memory, normalizer, stab, gain,
    heads, norm_out, stab_out, forget_out, key_out, value_out, *, model_width, total_heads,
):
    seqs, local = memory.shape[0], memory.shape[1]
    tp = lax.axis_index("tp")
    qw, vw = local * QK, local * VD

    def summed(lo, width):
        return jnp.sum(recv[:, :, lo : lo + width].astype(F32), axis=0)

    small = summed(2 * qw + 2 * vw, LANES)
    inverse = lax.rsqrt(small[:, 2 * total_heads : 2 * total_heads + 1] / model_width + EPSILON)
    query = (summed(0, qw) * inverse).astype(BF16).astype(F32)
    key = (summed(qw, qw) * (inverse * QK ** (-0.5))).astype(BF16).astype(F32)
    value = (summed(2 * qw, vw) * inverse).astype(BF16).astype(F32)
    outgate = (summed(2 * qw + vw, vw) * inverse).astype(BF16).astype(F32)
    row = lax.broadcasted_iota(jnp.int32, (seqs, QK), 0)
    diag = lax.broadcasted_iota(jnp.int32, (seqs, seqs), 0) == lax.broadcasted_iota(
        jnp.int32, (seqs, seqs), 1
    )

    def own(at, h):
        both = [small[:, at + t * local + h : at + t * local + h + 1] for t in range(total_heads // local)]
        got = both[0]
        for t in range(1, len(both)):
            got = jnp.where(tp == t, both[t], got)
        return got

    partial = []
    for h in range(local):
        input_pre = own(0, h) * inverse
        log_forget = jax.nn.log_sigmoid(own(total_heads, h) * inverse + bias[:, h : h + 1])
        old = jnp.sum(jnp.where(diag, stab[h : h + 1, :], 0.0), axis=1, keepdims=True)
        new = jnp.maximum(log_forget + old, input_pre)
        forget = jnp.exp(log_forget + old - new)
        scale = jnp.exp(input_pre - new)
        stab_out[h : h + 1, :] = jnp.sum(jnp.where(diag, new, 0.0), axis=0, keepdims=True)
        q, k = query[:, h * QK : (h + 1) * QK], key[:, h * QK : (h + 1) * QK]
        scaled_key = scale * k
        new_norm = forget * normalizer[:, h, :] + scaled_key
        norm_out[:, h, :] = new_norm
        v = value[:, h * VD : (h + 1) * VD]
        forget_out[:, h, :] = jnp.broadcast_to(forget, (seqs, LANES))
        key_out[:, h, :] = scaled_key
        value_out[:, h, :] = v
        denom = jnp.maximum(jnp.abs(jnp.sum(q * new_norm, axis=1, keepdims=True)), 1.0)
        query_key = jnp.sum(q * k, axis=1, keepdims=True)
        spread = [jnp.where(row == b, q, 0.0).astype(BF16) for b in range(seqs)]
        partial.append((forget, (scale * query_key) * v, denom, spread))
    for h in range(local):
        forget, fresh, denom, spread = partial[h]
        carried = jnp.zeros((seqs, VD), F32)
        for b in range(0, seqs, 2):
            left = jnp.concatenate([spread[b], spread[b + 1]], axis=1)
            right = jnp.concatenate([memory[b, h], memory[b + 1, h]], axis=0).astype(BF16)
            carried = carried + jnp.dot(left, right, preferred_element_type=F32)
        head_out = (forget * carried + fresh) / denom
        normed = head_out * lax.rsqrt(jnp.mean(head_out * head_out, axis=1, keepdims=True) + EPSILON)
        gate = jax.nn.sigmoid(outgate[:, h * VD : (h + 1) * VD])
        mixed = (normed * gain[h : h + 1, :] * gate).astype(BF16)
        heads[:, :, h * VD : (h + 1) * VD] = jnp.broadcast_to(mixed[None], (heads.shape[0], seqs, VD))


def state_step(recv, forget_bias, memory, normalizer, stabilizer, head_gain, model_width, total_heads):
    blocks = recv.shape[0]
    seqs, local = memory.shape[:2]

    def kernel(*refs):
        state_kernel(*refs, model_width=model_width, total_heads=total_heads)

    return pl.pallas_call(
        kernel,
        out_shape=(
            jax.ShapeDtypeStruct((blocks, seqs, local * VD), BF16),
            jax.ShapeDtypeStruct((seqs, local, QK), F32),
            jax.ShapeDtypeStruct((local, seqs), F32),
            jax.ShapeDtypeStruct((seqs, local, LANES), F32),
            jax.ShapeDtypeStruct((seqs, local, QK), F32),
            jax.ShapeDtypeStruct((seqs, local, VD), F32),
        ),
        in_specs=[spec(VMEM)] * 6,
        out_specs=[spec(VMEM)] * 6,
        compiler_params=pltpu.CompilerParams(vmem_limit_bytes=16 << 20),
        name="state",
    )(recv, forget_bias[None], memory, normalizer, stabilizer.T, head_gain)


def memory_kernel(memory, forget, key, value, *rest, first):
    target, fresh, sems = rest[-3:]
    seqs = memory.shape[0]
    writes = []
    for n in range(fresh.shape[0]):
        h = first + n
        key_cols = key[:, h, :].T
        for b in range(seqs):
            decay = forget[b : b + 1, h, :1]
            fresh[n, b] = decay * memory[b, h] + key_cols[:, b : b + 1] * value[b : b + 1, h, :]
        write = pltpu.make_async_copy(fresh.at[n], target.at[:, h], sems.at[n])
        write.start()
        writes.append(write)
    for write in writes:
        write.wait()


def memory_step(memory, forget, key, value, first, count, partial=None):
    def kernel(*refs):
        memory_kernel(*refs, first=first)

    extra = [] if partial is None else stay(partial)
    return pl.pallas_call(
        kernel,
        out_shape=HBM(memory.shape, F32),
        in_specs=[spec(VMEM)] * 4 + [spec(HBM)] * len(extra),
        out_specs=spec(HBM),
        input_output_aliases={4: 0} if extra else {},
        scratch_shapes=[
            pltpu.VMEM((count, memory.shape[0]) + memory.shape[2:], F32),
            pltpu.SemaphoreType.DMA((count,)),
        ],
        compiler_params=pltpu.CompilerParams(vmem_limit_bytes=6 << 20),
        name="memory",
    )(memory, forget, key, value, *extra)


def mixer_kernel(rows_ref, gain, wg, wu, wd, keep, give, mlp):
    blocks, rows, cols = rows_ref.shape
    tp = lax.axis_index("tp")
    total = jnp.zeros((rows, cols), F32)
    for j in range(blocks):
        value = rows_ref[j].astype(F32)
        total = total + value * value
    inverse = lax.rsqrt(jnp.sum(total, axis=1, keepdims=True) / (blocks * cols) + EPSILON)
    for j in range(blocks):
        lo = j * cols
        value = rows_ref[j].astype(F32) * inverse * gain[:, lo : lo + cols]
        mlp[:, lo : lo + cols] = value.astype(BF16)
    gate = lax.dot_general(mlp[...], wg[...], NT, preferred_element_type=F32)
    up = lax.dot_general(mlp[...], wu[...], NT, preferred_element_type=F32)
    hidden = (jax.nn.silu(gate) * up).astype(BF16)
    half = keep.shape[1]
    for j in range(blocks):
        part = jnp.dot(hidden, wd[:, j * cols : (j + 1) * cols], preferred_element_type=F32).T
        first, second = part[:half].astype(BF16), part[half:].astype(BF16)
        keep[j] = jnp.where(tp == 0, first, second)
        give[j] = jnp.where(tp == 0, second, first)


def mixer(gathered, mlp_gain, w_gate, w_up, w_down):
    blocks, rows, cols = gathered.shape
    half = jax.ShapeDtypeStruct((blocks, cols // 2, rows), BF16)
    return pl.pallas_call(
        mixer_kernel,
        out_shape=(half, half),
        in_specs=[spec(VMEM)] * 5,
        out_specs=[spec(VMEM)] * 2,
        scratch_shapes=[pltpu.VMEM((rows, blocks * cols), BF16)],
        compiler_params=pltpu.CompilerParams(vmem_limit_bytes=16 << 20),
        name="mixer",
    )(gathered, mlp_gain[None], w_gate.T, w_up.T, w_down)


def branch_kernel(heads, w_out, out):
    rows = heads[...].reshape(out.shape[0], w_out.shape[0])
    out[...] = jnp.dot(rows, w_out[...], preferred_element_type=F32).astype(BF16)


def branch_step(heads, w_out):
    return pl.pallas_call(
        branch_kernel,
        out_shape=jax.ShapeDtypeStruct((heads.shape[0] * heads.shape[1], w_out.shape[1]), BF16),
        in_specs=[spec(VMEM)] * 2,
        out_specs=spec(VMEM),
        compiler_params=pltpu.CompilerParams(vmem_limit_bytes=4 << 20),
        name="branch",
    )(heads, w_out)


def pair_kernel(keep, got, after, out):
    out[...] = (keep[...].astype(F32) + got[...].astype(F32)).astype(BF16)


def pair_step(keep, got, after):
    return pl.pallas_call(
        pair_kernel,
        out_shape=jax.ShapeDtypeStruct(keep.shape, BF16),
        in_specs=[spec(VMEM)] * 2 + [spec(HBM)],
        out_specs=spec(VMEM),
        compiler_params=pltpu.CompilerParams(vmem_limit_bytes=4 << 20),
        name="pair",
    )(keep, got, *stay(after))


def residual_kernel(tokens, branch, other, after, spread, own):
    total = tokens[...].astype(F32) + (branch[...].astype(F32) + other[...].astype(F32))
    rounded = total.astype(BF16)
    spread[...] = jnp.broadcast_to(rounded[None], spread.shape)
    turned = rounded.astype(F32).T
    half = own.shape[0]
    own[...] = jnp.where(lax.axis_index("tp") == 0, turned[:half], turned[half:]).astype(BF16)


def residual_step(tokens, branch, other, after, blocks):
    rows, cols = tokens.shape
    return pl.pallas_call(
        residual_kernel,
        out_shape=(
            jax.ShapeDtypeStruct((blocks, rows, cols), BF16),
            jax.ShapeDtypeStruct((cols // 2, rows), BF16),
        ),
        in_specs=[spec(VMEM)] * 3 + [spec(HBM)],
        out_specs=[spec(VMEM)] * 2,
        compiler_params=pltpu.CompilerParams(vmem_limit_bytes=4 << 20),
        name="residual",
    )(tokens, branch, other, *stay(after))


def finish_kernel(recv, own, out):
    out[...] = (jnp.sum(recv[...].astype(F32), axis=0) + own[...].astype(F32)).astype(BF16)


def finish(recv, own):
    return pl.pallas_call(
        finish_kernel,
        out_shape=jax.ShapeDtypeStruct(own.shape, BF16),
        in_specs=[spec(VMEM)] * 2,
        out_specs=spec(VMEM),
        compiler_params=pltpu.CompilerParams(vmem_limit_bytes=4 << 20),
        name="finish",
    )(recv, own)


def other_core(value):
    return lax.ppermute(value, "tp", [(0, 1), (1, 0)])


def exchanged(blocks):
    return lax.all_to_all(blocks, "kv", 0, 0, tiled=True)


def body(
    tokens,
    mix_gain,
    w_query,
    w_key,
    w_value,
    w_outgate,
    w_gates,
    forget_bias,
    memory,
    normalizer,
    stabilizer,
    head_gain,
    w_out,
    mlp_gain,
    w_gate,
    w_up,
    w_down,
):
    devices = lax.axis_size("kv")
    rows, block_cols = tokens.shape
    send = project(tokens, mix_gain, w_query, w_key, w_value, w_outgate, w_gates, devices)
    heads, new_normalizer, new_stabilizer, forget, key, value = state_step(
        exchanged(send),
        forget_bias,
        memory,
        normalizer,
        stabilizer,
        head_gain,
        block_cols * devices,
        w_gates.shape[1] // 2,
    )
    branch = branch_step(exchanged(heads), w_out)
    half = memory.shape[1] // 2
    forget, key, value, _ = lax.optimization_barrier((forget, key, value, branch))
    first_half = memory_step(memory, forget, key, value, 0, half)
    spread, own = residual_step(tokens, branch, other_core(branch), first_half, devices)
    gathered = exchanged(spread)
    keep, give = mixer(gathered, mlp_gain, w_gate, w_up, w_down)
    forget, key, value, _ = lax.optimization_barrier((forget, key, value, give))
    new_memory = memory_step(memory, forget, key, value, half, half, first_half)
    pair = pair_step(keep, other_core(give), new_memory)
    mixed_out = finish(exchanged(pair), own).T
    return (mixed_out, new_memory, new_normalizer, new_stabilizer.T)


def solution(mesh):
    in_specs = (
        P("dp", "kv"),
        P("kv"),
        P("kv", "tp"),
        P("kv", "tp"),
        P("kv", "tp"),
        P("kv", "tp"),
        P(),
        P("tp"),
        P(("dp", "kv"), "tp", None, None),
        P(("dp", "kv"), "tp", None),
        P(("dp", "kv"), "tp"),
        P("tp", None),
        P("tp", "kv"),
        P(),
        P(None, ("kv", "tp")),
        P(None, ("kv", "tp")),
        P(("kv", "tp"), None),
    )
    out_specs = (
        P("dp", ("kv", "tp")),
        P(("dp", "kv"), "tp", None, None),
        P(("dp", "kv"), "tp", None),
        P(("dp", "kv"), "tp"),
    )
    return jax.shard_map(body, mesh=mesh, in_specs=in_specs, out_specs=out_specs, check_vma=False)
```

```python
import jax
import jax.numpy as jnp
from jax import lax
from jax.experimental import pallas as pl
from jax.experimental.pallas import tpu as pltpu
from jax.sharding import PartitionSpec as P

QK = 128
VD = 256
EPSILON = 1e-06
LANES = 128
SUBLANES = 8
F32 = jnp.float32
BF16 = jnp.bfloat16
NT = (((1,), (1,)), ((), ()))
VMEM = pltpu.MemorySpace.VMEM
SMEM = pltpu.MemorySpace.SMEM
HBM = pltpu.MemorySpace.HBM


def spec(space):
    return pl.BlockSpec(memory_space=space)


def stay(*arrays):
    return [pltpu.with_memory_space_constraint(a, HBM) for a in arrays]


def fetch(pairs, sems):
    copies = [pltpu.make_async_copy(src, dst, sems.at[n]) for n, (src, dst) in enumerate(pairs)]
    for copy in copies:
        copy.start()
    return copies


def project_kernel(tokens, gain, wq, wk, wv, wo, wg, out, bt, bn, bq, bk, bv, bo, bg, sems):
    cols = tokens.shape[1]
    kv = lax.axis_index("kv")
    gate_src = wg.at[:, pl.ds(pl.multiple_of(kv * cols, LANES), cols)]
    copies = fetch(
        ((tokens, bt), (gain, bn), (wq, bq), (wk, bk), (gate_src, bg), (wv, bv), (wo, bo)), sems
    )
    blocks, rows = out.shape[:2]
    copies[0].wait()
    copies[1].wait()
    act = bt[...].astype(F32)
    square = jnp.sum(act * act, axis=1, keepdims=True)
    scaled = (act * bn[...]).astype(BF16)

    def put(value, at):
        width = value.shape[1]
        out[:, :, at : at + width] = value.reshape(blocks, rows, width).astype(BF16)

    at = 0
    for n, buf in ((2, bq), (3, bk), (5, bv), (6, bo)):
        copies[n].wait()
        put(jnp.dot(scaled, buf[...], preferred_element_type=F32), at)
        at += buf.shape[1]
    copies[4].wait()
    gate_count = bg.shape[0]
    wide = jnp.concatenate([bg[...].astype(F32), jnp.zeros((LANES - gate_count, cols), F32)], axis=0)
    gates = lax.dot_general(scaled, wide.astype(BF16), NT, preferred_element_type=F32)
    lane = lax.broadcasted_iota(jnp.int32, gates.shape, 1)
    put(jnp.where(lane == gate_count, square, gates), at)


def project(tokens, mix_gain, w_query, w_key, w_value, w_outgate, w_gates, blocks):
    rows, cols = tokens.shape
    width = w_query.shape[1] + w_key.shape[1] + w_value.shape[1] + w_outgate.shape[1] + LANES
    weights = (w_query, w_key, w_value, w_outgate)
    return pl.pallas_call(
        project_kernel,
        out_shape=jax.ShapeDtypeStruct((blocks, rows // blocks, width), BF16),
        in_specs=[spec(HBM)] * 7,
        out_specs=spec(VMEM),
        scratch_shapes=[pltpu.VMEM((rows, cols), BF16), pltpu.VMEM((1, cols), F32)]
        + [pltpu.VMEM(w.shape, BF16) for w in weights]
        + [pltpu.VMEM((w_gates.shape[1], cols), BF16), pltpu.SemaphoreType.DMA((7,))],
        compiler_params=pltpu.CompilerParams(vmem_limit_bytes=8 << 20),
        cost_estimate=pl.CostEstimate(flops=10**10, bytes_accessed=10**7, transcendentals=0),
        name="project",
    )(*stay(tokens, mix_gain[None], *weights, w_gates.T))


def state_kernel(
    recv, bias, memory, normalizer, stab, gain,
    heads, norm_out, stab_out, forget_out, key_out, value_out, *, model_width, total_heads,
):
    seqs, local = memory.shape[0], memory.shape[1]
    tp = lax.axis_index("tp")
    qw, vw = local * QK, local * VD

    def summed(lo, width):
        return jnp.sum(recv[:, :, lo : lo + width].astype(F32), axis=0)

    small = summed(2 * qw + 2 * vw, LANES)
    inverse = lax.rsqrt(small[:, 2 * total_heads : 2 * total_heads + 1] / model_width + EPSILON)
    query = (summed(0, qw) * inverse).astype(BF16).astype(F32)
    key = (summed(qw, qw) * (inverse * QK ** (-0.5))).astype(BF16).astype(F32)
    value = (summed(2 * qw, vw) * inverse).astype(BF16).astype(F32)
    outgate = (summed(2 * qw + vw, vw) * inverse).astype(BF16).astype(F32)
    row = lax.broadcasted_iota(jnp.int32, (seqs, QK), 0)
    diag = lax.broadcasted_iota(jnp.int32, (seqs, seqs), 0) == lax.broadcasted_iota(
        jnp.int32, (seqs, seqs), 1
    )

    def own(at, h):
        both = [small[:, at + t * local + h : at + t * local + h + 1] for t in range(total_heads // local)]
        got = both[0]
        for t in range(1, len(both)):
            got = jnp.where(tp == t, both[t], got)
        return got

    partial = []
    for h in range(local):
        input_pre = own(0, h) * inverse
        log_forget = jax.nn.log_sigmoid(own(total_heads, h) * inverse + bias[:, h : h + 1])
        old = jnp.sum(jnp.where(diag, stab[h : h + 1, :], 0.0), axis=1, keepdims=True)
        new = jnp.maximum(log_forget + old, input_pre)
        forget = jnp.exp(log_forget + old - new)
        scale = jnp.exp(input_pre - new)
        stab_out[h : h + 1, :] = jnp.sum(jnp.where(diag, new, 0.0), axis=0, keepdims=True)
        q, k = query[:, h * QK : (h + 1) * QK], key[:, h * QK : (h + 1) * QK]
        scaled_key = scale * k
        new_norm = forget * normalizer[:, h, :] + scaled_key
        norm_out[:, h, :] = new_norm
        v = value[:, h * VD : (h + 1) * VD]
        forget_out[:, h, :] = jnp.broadcast_to(forget, (seqs, LANES))
        key_out[:, h, :] = scaled_key
        value_out[:, h, :] = v
        denom = jnp.maximum(jnp.abs(jnp.sum(q * new_norm, axis=1, keepdims=True)), 1.0)
        query_key = jnp.sum(q * k, axis=1, keepdims=True)
        spread = [jnp.where(row == b, q, 0.0).astype(BF16) for b in range(seqs)]
        partial.append((forget, (scale * query_key) * v, denom, spread))
    for h in range(local):
        forget, fresh, denom, spread = partial[h]
        carried = jnp.zeros((seqs, VD), F32)
        for b in range(0, seqs, 2):
            left = jnp.concatenate([spread[b], spread[b + 1]], axis=1)
            right = jnp.concatenate([memory[b, h], memory[b + 1, h]], axis=0).astype(BF16)
            carried = carried + jnp.dot(left, right, preferred_element_type=F32)
        head_out = (forget * carried + fresh) / denom
        normed = head_out * lax.rsqrt(jnp.mean(head_out * head_out, axis=1, keepdims=True) + EPSILON)
        gate = jax.nn.sigmoid(outgate[:, h * VD : (h + 1) * VD])
        mixed = (normed * gain[h : h + 1, :] * gate).astype(BF16)
        heads[:, :, h * VD : (h + 1) * VD] = jnp.broadcast_to(mixed[None], (heads.shape[0], seqs, VD))


def state_step(recv, forget_bias, memory, normalizer, stabilizer, head_gain, model_width, total_heads):
    blocks = recv.shape[0]
    seqs, local = memory.shape[:2]

    def kernel(*refs):
        state_kernel(*refs, model_width=model_width, total_heads=total_heads)

    return pl.pallas_call(
        kernel,
        out_shape=(
            jax.ShapeDtypeStruct((blocks, seqs, local * VD), BF16),
            jax.ShapeDtypeStruct((seqs, local, QK), F32),
            jax.ShapeDtypeStruct((local, seqs), F32),
            jax.ShapeDtypeStruct((seqs, local, LANES), F32),
            jax.ShapeDtypeStruct((seqs, local, QK), F32),
            jax.ShapeDtypeStruct((seqs, local, VD), F32),
        ),
        in_specs=[spec(VMEM)] * 6,
        out_specs=[spec(VMEM)] * 6,
        compiler_params=pltpu.CompilerParams(vmem_limit_bytes=16 << 20),
        name="state",
    )(recv, forget_bias[None], memory, normalizer, stabilizer.T, head_gain)


def memory_kernel(*refs, first, count, kept):
    memory, forget, key, value = refs[:4]
    small = refs[4 : 4 + kept]
    target = refs[-3 - kept]
    small_out = refs[len(refs) - 2 - kept : len(refs) - 2]
    fresh, sems = refs[-2:]
    seqs = memory.shape[0]
    writes = []

    def send(src, dst):
        write = pltpu.make_async_copy(src, dst, sems.at[len(writes)])
        write.start()
        writes.append(write)

    for src, dst in zip(small, small_out):
        send(src, dst)
    for n in range(count):
        h = first + n
        key_cols = key[:, h, :].T
        for b in range(seqs):
            decay = forget[b : b + 1, h, :1]
            fresh[n, b] = decay * memory[b, h] + key_cols[:, b : b + 1] * value[b : b + 1, h, :]
            if b % 2:
                send(fresh.at[n, b - 1 : b + 1], target.at[b - 1 : b + 1, h])
    for write in writes:
        write.wait()


def memory_step(memory, forget, key, value, first, count, partial=None, small=()):
    def kernel(*refs):
        memory_kernel(*refs, first=first, count=count, kept=len(small))

    extra = [] if partial is None else stay(partial)
    outs = [HBM(memory.shape, F32)] + [HBM(a.shape, F32) for a in small]
    got = pl.pallas_call(
        kernel,
        out_shape=outs,
        in_specs=[spec(VMEM)] * (4 + len(small)) + [spec(HBM)] * len(extra),
        out_specs=[spec(HBM)] * len(outs),
        input_output_aliases={4: 0} if extra else {},
        scratch_shapes=[
            pltpu.VMEM((count, memory.shape[0]) + memory.shape[2:], F32),
            pltpu.SemaphoreType.DMA((count * memory.shape[0] // 2 + len(small),)),
        ],
        compiler_params=pltpu.CompilerParams(vmem_limit_bytes=6 << 20),
        cost_estimate=pl.CostEstimate(flops=0, bytes_accessed=0, transcendentals=0),
        name="memory",
    )(memory, forget, key, value, *small, *extra)
    return got if small else got[0]


def mixer_kernel(mine, other, after, wg, wu, wd, keep, give, mlp):
    blocks, tall, rows = mine.shape
    half = keep.shape[1]
    cols = 2 * half
    tp = lax.axis_index("tp")
    low = tp == 0
    square = jnp.zeros((tall - half, rows), F32)
    for j in range(blocks):
        square = square + (mine[j, half:].astype(F32) + other[j, half:].astype(F32))
        mlp[pl.ds(pl.multiple_of(j * cols + tp * half, half), half), :] = mine[j, :half]
        mlp[pl.ds(pl.multiple_of(j * cols + (1 - tp) * half, half), half), :] = other[j, :half]
    inverse = lax.rsqrt(jnp.sum(square, axis=0, keepdims=True) / (blocks * cols) + EPSILON)
    gate = jnp.dot(wg[...], mlp[...], preferred_element_type=F32) * inverse
    up = jnp.dot(wu[...], mlp[...], preferred_element_type=F32) * inverse
    hidden = (jax.nn.silu(gate) * up).T.astype(BF16)
    for j in range(blocks):
        part = jnp.dot(hidden, wd[:, j * cols : (j + 1) * cols], preferred_element_type=F32).T
        first, second = part[:half].astype(BF16), part[half:].astype(BF16)
        keep[j] = jnp.where(low, first, second)
        give[j] = jnp.where(low, second, first)


def mixer(mine, other, after, w_gate, w_up, w_down, half):
    blocks, _, rows = mine.shape
    result = jax.ShapeDtypeStruct((blocks, half, rows), BF16)
    return pl.pallas_call(
        mixer_kernel,
        out_shape=(result, result),
        in_specs=[spec(VMEM)] * 2 + [spec(HBM)] + [spec(VMEM)] * 3,
        out_specs=[spec(VMEM)] * 2,
        scratch_shapes=[pltpu.VMEM((2 * blocks * half, rows), BF16)],
        compiler_params=pltpu.CompilerParams(vmem_limit_bytes=16 << 20),
        name="mixer",
    )(mine, other, *stay(after), w_gate.T, w_up.T, w_down)


def halves(turned):
    half = turned.shape[0] // 2
    low = lax.axis_index("tp") == 0
    first, second = turned[:half], turned[half:]
    return jnp.where(low, first, second), jnp.where(low, second, first)


def branch_kernel(heads, w_out, wg, wu, wd, keep, give):
    rows = heads[...].reshape(heads.shape[0] * heads.shape[1], w_out.shape[0])
    mine, other = halves(jnp.dot(rows, w_out[...], preferred_element_type=F32).T)
    keep[...] = mine.astype(BF16)
    give[...] = other.astype(BF16)


def branch_step(heads, w_out, *early):
    result = jax.ShapeDtypeStruct((w_out.shape[1] // 2, heads.shape[0] * heads.shape[1]), BF16)
    return pl.pallas_call(
        branch_kernel,
        out_shape=(result, result),
        in_specs=[spec(VMEM)] * (2 + len(early)),
        out_specs=[spec(VMEM)] * 2,
        compiler_params=pltpu.CompilerParams(vmem_limit_bytes=4 << 20),
        name="branch",
    )(heads, w_out, *early)


def pair_kernel(keep, got, after, out):
    out[...] = (keep[...].astype(F32) + got[...].astype(F32)).astype(BF16)


def pair_step(keep, got, after):
    return pl.pallas_call(
        pair_kernel,
        out_shape=jax.ShapeDtypeStruct(keep.shape, BF16),
        in_specs=[spec(VMEM)] * 2 + [spec(HBM)],
        out_specs=spec(VMEM),
        compiler_params=pltpu.CompilerParams(vmem_limit_bytes=4 << 20),
        name="pair",
    )(keep, got, *stay(after))


def residual_kernel(tokens, keep, got, gain, after, spread, own):
    half, rows = own.shape
    mine, _ = halves(tokens[...].astype(F32).T)
    column, _ = halves(gain[pl.ds(lax.axis_index("kv"), 1), :].T)
    rounded = (mine + (keep[...].astype(F32) + got[...].astype(F32))).astype(BF16)
    own[...] = rounded
    value = rounded.astype(F32)
    square = jnp.sum(value * value, axis=0, keepdims=True)
    coarse = square.astype(BF16).astype(F32)
    line = lax.broadcasted_iota(jnp.int32, (spread.shape[1] - half, rows), 0)
    tail = jnp.where(line == 0, coarse, jnp.where(line == 1, square - coarse, 0.0))
    scaled = (value * column).astype(BF16)
    spread[:, :half] = jnp.broadcast_to(scaled[None], (spread.shape[0], half, rows))
    spread[:, half:] = jnp.broadcast_to(tail.astype(BF16)[None], (spread.shape[0],) + tail.shape)


def residual_step(tokens, keep, got, mlp_gain, after, blocks):
    half, rows = keep.shape
    return pl.pallas_call(
        residual_kernel,
        out_shape=(
            jax.ShapeDtypeStruct((blocks, half + SUBLANES, rows), BF16),
            jax.ShapeDtypeStruct(keep.shape, BF16),
        ),
        in_specs=[spec(VMEM)] * 4 + [spec(HBM)],
        out_specs=[spec(VMEM)] * 2,
        compiler_params=pltpu.CompilerParams(vmem_limit_bytes=4 << 20),
        name="residual",
    )(tokens, keep, got, mlp_gain.reshape(blocks, 2 * half), *stay(after))


def finish_kernel(recv, own, out):
    out[...] = (jnp.sum(recv[...].astype(F32), axis=0) + own[...].astype(F32)).astype(BF16)


def finish(recv, own):
    return pl.pallas_call(
        finish_kernel,
        out_shape=jax.ShapeDtypeStruct(own.shape, BF16),
        in_specs=[spec(VMEM)] * 2,
        out_specs=spec(VMEM),
        compiler_params=pltpu.CompilerParams(vmem_limit_bytes=4 << 20),
        name="finish",
    )(recv, own)


def other_core(value):
    return lax.ppermute(value, "tp", [(0, 1), (1, 0)])


def exchanged(blocks):
    return lax.all_to_all(blocks, "kv", 0, 0, tiled=True)


def body(
    tokens,
    mix_gain,
    w_query,
    w_key,
    w_value,
    w_outgate,
    w_gates,
    forget_bias,
    memory,
    normalizer,
    stabilizer,
    head_gain,
    w_out,
    mlp_gain,
    w_gate,
    w_up,
    w_down,
):
    devices = lax.axis_size("kv")
    rows, block_cols = tokens.shape
    send = project(tokens, mix_gain, w_query, w_key, w_value, w_outgate, w_gates, devices)
    heads, new_normalizer, new_stabilizer, forget, key, value_heads = state_step(
        exchanged(send),
        forget_bias,
        memory,
        normalizer,
        stabilizer,
        head_gain,
        block_cols * devices,
        w_gates.shape[1] // 2,
    )
    def behind(value):
        return lax.optimization_barrier((forget, key, value_heads, value))[:3]

    keep, give = branch_step(exchanged(heads), w_out, w_gate.T, w_up.T, w_down)
    part, new_normalizer, new_stabilizer = memory_step(
        memory, *behind(give), 0, 1, small=(new_normalizer, new_stabilizer)
    )
    spread, own = residual_step(tokens, keep, other_core(give), mlp_gain, part, devices)
    mine = exchanged(spread)
    part = memory_step(memory, *behind(mine), 1, 1, part)
    keep, give = mixer(mine, other_core(mine), part, w_gate, w_up, w_down, own.shape[0])
    new_memory = memory_step(memory, *behind(give), 2, memory.shape[1] - 2, part)
    pair = pair_step(keep, other_core(give), new_memory)
    mixed_out = finish(exchanged(pair), own).T
    return (mixed_out, new_memory, new_normalizer, new_stabilizer.T)


def solution(mesh):
    in_specs = (
        P("dp", "kv"),
        P("kv"),
        P("kv", "tp"),
        P("kv", "tp"),
        P("kv", "tp"),
        P("kv", "tp"),
        P(),
        P("tp"),
        P(("dp", "kv"), "tp", None, None),
        P(("dp", "kv"), "tp", None),
        P(("dp", "kv"), "tp"),
        P("tp", None),
        P("tp", "kv"),
        P(),
        P(None, ("kv", "tp")),
        P(None, ("kv", "tp")),
        P(("kv", "tp"), None),
    )
    out_specs = (
        P("dp", ("kv", "tp")),
        P(("dp", "kv"), "tp", None, None),
        P(("dp", "kv"), "tp", None),
        P(("dp", "kv"), "tp"),
    )
    return jax.shard_map(body, mesh=mesh, in_specs=in_specs, out_specs=out_specs, check_vma=False)
```

```python
import jax
import jax.numpy as jnp
from jax import lax
from jax.experimental import pallas as pl
from jax.experimental.pallas import tpu as pltpu
from jax.sharding import PartitionSpec as P

QK = 128
VD = 256
EPSILON = 1e-06
LANES = 128
F32 = jnp.float32
BF16 = jnp.bfloat16
NT = (((1,), (1,)), ((), ()))
VMEM = pltpu.MemorySpace.VMEM
SMEM = pltpu.MemorySpace.SMEM
HBM = pltpu.MemorySpace.HBM


def spec(space):
    return pl.BlockSpec(memory_space=space)


def stay(*arrays):
    return [pltpu.with_memory_space_constraint(a, HBM) for a in arrays]


def fetch(pairs, sems):
    copies = [pltpu.make_async_copy(src, dst, sems.at[n]) for n, (src, dst) in enumerate(pairs)]
    for copy in copies:
        copy.start()
    return copies


def project_kernel(tokens, gain, wq, wk, wv, wo, wg, out, bt, bn, bq, bk, bv, bo, bg, sems):
    cols = tokens.shape[1]
    kv = lax.axis_index("kv")
    gate_src = wg.at[:, pl.ds(pl.multiple_of(kv * cols, LANES), cols)]
    copies = fetch(
        ((tokens, bt), (gain, bn), (wq, bq), (wk, bk), (gate_src, bg), (wv, bv), (wo, bo)), sems
    )
    blocks, rows = out.shape[:2]
    copies[0].wait()
    copies[1].wait()
    act = bt[...].astype(F32)
    square = jnp.sum(act * act, axis=1, keepdims=True)
    scaled = (act * bn[...]).astype(BF16)

    def put(value, at):
        width = value.shape[1]
        out[:, :, at : at + width] = value.reshape(blocks, rows, width).astype(BF16)

    at = 0
    for n, buf in ((2, bq), (3, bk), (5, bv), (6, bo)):
        copies[n].wait()
        put(jnp.dot(scaled, buf[...], preferred_element_type=F32), at)
        at += buf.shape[1]
    copies[4].wait()
    gate_count = bg.shape[0]
    wide = jnp.concatenate([bg[...].astype(F32), jnp.zeros((LANES - gate_count, cols), F32)], axis=0)
    gates = lax.dot_general(scaled, wide.astype(BF16), NT, preferred_element_type=F32)
    lane = lax.broadcasted_iota(jnp.int32, gates.shape, 1)
    put(jnp.where(lane == gate_count, square, gates), at)


def project(tokens, mix_gain, w_query, w_key, w_value, w_outgate, w_gates, blocks):
    rows, cols = tokens.shape
    width = w_query.shape[1] + w_key.shape[1] + w_value.shape[1] + w_outgate.shape[1] + LANES
    weights = (w_query, w_key, w_value, w_outgate)
    return pl.pallas_call(
        project_kernel,
        out_shape=jax.ShapeDtypeStruct((blocks, rows // blocks, width), BF16),
        in_specs=[spec(HBM)] * 7,
        out_specs=spec(VMEM),
        scratch_shapes=[pltpu.VMEM((rows, cols), BF16), pltpu.VMEM((1, cols), F32)]
        + [pltpu.VMEM(w.shape, BF16) for w in weights]
        + [pltpu.VMEM((w_gates.shape[1], cols), BF16), pltpu.SemaphoreType.DMA((7,))],
        compiler_params=pltpu.CompilerParams(vmem_limit_bytes=8 << 20),
        cost_estimate=pl.CostEstimate(flops=10**10, bytes_accessed=10**7, transcendentals=0),
        name="project",
    )(*stay(tokens, mix_gain[None], *weights, w_gates.T))


def state_kernel(
    recv, bias, memory, normalizer, stab, gain,
    heads, norm_out, stab_out, forget_out, key_out, value_out, *, model_width, total_heads,
):
    seqs, local = memory.shape[0], memory.shape[1]
    tp = lax.axis_index("tp")
    qw, vw = local * QK, local * VD

    def summed(lo, width):
        return jnp.sum(recv[:, :, lo : lo + width].astype(F32), axis=0)

    small = summed(2 * qw + 2 * vw, LANES)
    inverse = lax.rsqrt(small[:, 2 * total_heads : 2 * total_heads + 1] / model_width + EPSILON)
    query = (summed(0, qw) * inverse).astype(BF16).astype(F32)
    key = (summed(qw, qw) * (inverse * QK ** (-0.5))).astype(BF16).astype(F32)
    value = (summed(2 * qw, vw) * inverse).astype(BF16).astype(F32)
    outgate = (summed(2 * qw + vw, vw) * inverse).astype(BF16).astype(F32)
    row = lax.broadcasted_iota(jnp.int32, (seqs, QK), 0)
    diag = lax.broadcasted_iota(jnp.int32, (seqs, seqs), 0) == lax.broadcasted_iota(
        jnp.int32, (seqs, seqs), 1
    )

    def own(at, h):
        both = [small[:, at + t * local + h : at + t * local + h + 1] for t in range(total_heads // local)]
        got = both[0]
        for t in range(1, len(both)):
            got = jnp.where(tp == t, both[t], got)
        return got

    partial = []
    for h in range(local):
        input_pre = own(0, h) * inverse
        log_forget = jax.nn.log_sigmoid(own(total_heads, h) * inverse + bias[:, h : h + 1])
        old = jnp.sum(jnp.where(diag, stab[h : h + 1, :], 0.0), axis=1, keepdims=True)
        new = jnp.maximum(log_forget + old, input_pre)
        forget = jnp.exp(log_forget + old - new)
        scale = jnp.exp(input_pre - new)
        stab_out[h : h + 1, :] = jnp.sum(jnp.where(diag, new, 0.0), axis=0, keepdims=True)
        q, k = query[:, h * QK : (h + 1) * QK], key[:, h * QK : (h + 1) * QK]
        scaled_key = scale * k
        new_norm = forget * normalizer[:, h, :] + scaled_key
        norm_out[:, h, :] = new_norm
        v = value[:, h * VD : (h + 1) * VD]
        forget_out[:, h, :] = jnp.broadcast_to(forget, (seqs, LANES))
        key_out[:, h, :] = scaled_key
        value_out[:, h, :] = v
        denom = jnp.maximum(jnp.abs(jnp.sum(q * new_norm, axis=1, keepdims=True)), 1.0)
        query_key = jnp.sum(q * k, axis=1, keepdims=True)
        spread = [jnp.where(row == b, q, 0.0).astype(BF16) for b in range(seqs)]
        partial.append((forget, (scale * query_key) * v, denom, spread))
    for h in range(local):
        forget, fresh, denom, spread = partial[h]
        carried = jnp.zeros((seqs, VD), F32)
        for b in range(0, seqs, 2):
            left = jnp.concatenate([spread[b], spread[b + 1]], axis=1)
            right = jnp.concatenate([memory[b, h], memory[b + 1, h]], axis=0).astype(BF16)
            carried = carried + jnp.dot(left, right, preferred_element_type=F32)
        head_out = (forget * carried + fresh) / denom
        normed = head_out * lax.rsqrt(jnp.mean(head_out * head_out, axis=1, keepdims=True) + EPSILON)
        gate = jax.nn.sigmoid(outgate[:, h * VD : (h + 1) * VD])
        mixed = (normed * gain[h : h + 1, :] * gate).astype(BF16)
        heads[:, :, h * VD : (h + 1) * VD] = jnp.broadcast_to(mixed[None], (heads.shape[0], seqs, VD))


def state_step(recv, forget_bias, memory, normalizer, stabilizer, head_gain, model_width, total_heads):
    blocks = recv.shape[0]
    seqs, local = memory.shape[:2]

    def kernel(*refs):
        state_kernel(*refs, model_width=model_width, total_heads=total_heads)

    return pl.pallas_call(
        kernel,
        out_shape=(
            jax.ShapeDtypeStruct((blocks, seqs, local * VD), BF16),
            jax.ShapeDtypeStruct((seqs, local, QK), F32),
            jax.ShapeDtypeStruct((local, seqs), F32),
            jax.ShapeDtypeStruct((seqs, local, LANES), F32),
            jax.ShapeDtypeStruct((seqs, local, QK), F32),
            jax.ShapeDtypeStruct((seqs, local, VD), F32),
        ),
        in_specs=[spec(VMEM)] * 6,
        out_specs=[spec(VMEM)] * 6,
        compiler_params=pltpu.CompilerParams(vmem_limit_bytes=16 << 20),
        name="state",
    )(recv, forget_bias[None], memory, normalizer, stabilizer.T, head_gain)


def memory_kernel(*refs, first, count, kept, scaled):
    memory, forget, key, value = refs[:4]
    small = refs[4 : 4 + kept]
    gain, *weights = refs[4 + kept : 5 + kept + scaled] if scaled else (None,)
    outs = refs[-3 - kept - scaled : -2]
    fresh, sems = refs[-2:]
    target, small_out, scaled_out = outs[0], outs[1 : 1 + kept], outs[1 + kept :]
    seqs = memory.shape[0]
    writes = []

    def send(src, dst):
        write = pltpu.make_async_copy(src, dst, sems.at[len(writes)])
        write.start()
        writes.append(write)

    for src, dst in zip(small, small_out):
        send(src, dst)
    key_cols = {}
    for n in range(count):
        h, b = divmod(first + n, seqs)
        if h not in key_cols:
            key_cols[h] = key[:, h, :].T
        decay = forget[b : b + 1, h, :1]
        fresh[n] = decay * memory[b, h] + key_cols[h][:, b : b + 1] * value[b : b + 1, h, :]
        send(fresh.at[n], target.at[b, h])
    for src, dst in zip(weights, scaled_out):
        dst[...] = (src[...].astype(F32) * gain[...]).astype(BF16)
    for write in writes:
        write.wait()


def memory_step(memory, forget, key, value, first, count, partial=None, small=(), gain=None, weights=()):
    def kernel(*refs):
        memory_kernel(*refs, first=first, count=count, kept=len(small), scaled=len(weights))

    near = [memory, forget, key, value, *small] + ([gain, *weights] if weights else [])
    extra = [] if partial is None else stay(partial)
    outs = [HBM(memory.shape, F32)] + [HBM(a.shape, F32) for a in small]
    kinds = [spec(HBM)] * len(outs) + [spec(VMEM)] * len(weights)
    outs += [jax.ShapeDtypeStruct(w.shape, BF16) for w in weights]
    return pl.pallas_call(
        kernel,
        out_shape=outs,
        in_specs=[spec(VMEM)] * len(near) + [spec(HBM)] * len(extra),
        out_specs=kinds,
        input_output_aliases={len(near): 0} if extra else {},
        scratch_shapes=[
            pltpu.VMEM((count,) + memory.shape[2:], F32),
            pltpu.SemaphoreType.DMA((count + len(small),)),
        ],
        compiler_params=pltpu.CompilerParams(vmem_limit_bytes=6 << 20),
        cost_estimate=pl.CostEstimate(flops=0, bytes_accessed=0, transcendentals=0),
        name="memory",
    )(*near, *extra)


def mixer_kernel(mine, other, after, wg, wu, wd, keep, give, mlp):
    blocks, half, rows = mine.shape
    cols = 2 * half
    tp = lax.axis_index("tp")
    low = tp == 0
    square = jnp.zeros((half, rows), F32)
    for j in range(blocks):
        mlp[pl.ds(pl.multiple_of(j * cols + tp * half, half), half), :] = mine[j]
        mlp[pl.ds(pl.multiple_of(j * cols + (1 - tp) * half, half), half), :] = other[j]
    for j in range(blocks):
        here, there = mine[j].astype(F32), other[j].astype(F32)
        square = square + (here * here + there * there)
    inverse = lax.rsqrt(jnp.sum(square, axis=0, keepdims=True) / (blocks * cols) + EPSILON)
    gate = jnp.dot(wg[...], mlp[...], preferred_element_type=F32) * inverse
    up = jnp.dot(wu[...], mlp[...], preferred_element_type=F32) * inverse
    hidden = (jax.nn.silu(gate) * up).T.astype(BF16)
    for j in range(blocks):
        part = jnp.dot(hidden, wd[:, j * cols : (j + 1) * cols], preferred_element_type=F32).T
        first, second = part[:half].astype(BF16), part[half:].astype(BF16)
        keep[j] = jnp.where(low, first, second)
        give[j] = jnp.where(low, second, first)


def mixer(mine, other, after, gate_rows, up_rows, w_down):
    blocks, half, rows = mine.shape
    result = jax.ShapeDtypeStruct((blocks, half, rows), BF16)
    return pl.pallas_call(
        mixer_kernel,
        out_shape=(result, result),
        in_specs=[spec(VMEM)] * 2 + [spec(HBM)] + [spec(VMEM)] * 3,
        out_specs=[spec(VMEM)] * 2,
        scratch_shapes=[pltpu.VMEM((2 * blocks * half, rows), BF16)],
        compiler_params=pltpu.CompilerParams(vmem_limit_bytes=16 << 20),
        name="mixer",
    )(mine, other, *stay(after), gate_rows, up_rows, w_down)


def halves(turned):
    half = turned.shape[0] // 2
    low = lax.axis_index("tp") == 0
    first, second = turned[:half], turned[half:]
    return jnp.where(low, first, second), jnp.where(low, second, first)


def branch_kernel(heads, w_out, wg, wu, wd, keep, give):
    rows = heads[...].reshape(heads.shape[0] * heads.shape[1], w_out.shape[0])
    mine, other = halves(jnp.dot(rows, w_out[...], preferred_element_type=F32).T)
    keep[...] = mine.astype(BF16)
    give[...] = other.astype(BF16)


def branch_step(heads, w_out, *early):
    result = jax.ShapeDtypeStruct((w_out.shape[1] // 2, heads.shape[0] * heads.shape[1]), BF16)
    return pl.pallas_call(
        branch_kernel,
        out_shape=(result, result),
        in_specs=[spec(VMEM)] * (2 + len(early)),
        out_specs=[spec(VMEM)] * 2,
        compiler_params=pltpu.CompilerParams(vmem_limit_bytes=4 << 20),
        name="branch",
    )(heads, w_out, *early)


def pair_kernel(keep, got, after, out):
    out[...] = (keep[...].astype(F32) + got[...].astype(F32)).astype(BF16)


def pair_step(keep, got, after):
    return pl.pallas_call(
        pair_kernel,
        out_shape=jax.ShapeDtypeStruct(keep.shape, BF16),
        in_specs=[spec(VMEM)] * 2 + [spec(HBM)],
        out_specs=spec(VMEM),
        compiler_params=pltpu.CompilerParams(vmem_limit_bytes=4 << 20),
        name="pair",
    )(keep, got, *stay(after))


def residual_kernel(tokens, keep, got, after, spread, own):
    mine, _ = halves(tokens[...].astype(F32).T)
    rounded = (mine + (keep[...].astype(F32) + got[...].astype(F32))).astype(BF16)
    own[...] = rounded
    spread[...] = jnp.broadcast_to(rounded[None], spread.shape)


def residual_step(tokens, keep, got, after, blocks):
    return pl.pallas_call(
        residual_kernel,
        out_shape=(
            jax.ShapeDtypeStruct((blocks,) + keep.shape, BF16),
            jax.ShapeDtypeStruct(keep.shape, BF16),
        ),
        in_specs=[spec(VMEM)] * 3 + [spec(HBM)],
        out_specs=[spec(VMEM)] * 2,
        compiler_params=pltpu.CompilerParams(vmem_limit_bytes=4 << 20),
        name="residual",
    )(tokens, keep, got, *stay(after))


def finish_kernel(recv, own, out):
    out[...] = (jnp.sum(recv[...].astype(F32), axis=0) + own[...].astype(F32)).astype(BF16)


def finish(recv, own):
    return pl.pallas_call(
        finish_kernel,
        out_shape=jax.ShapeDtypeStruct(own.shape, BF16),
        in_specs=[spec(VMEM)] * 2,
        out_specs=spec(VMEM),
        compiler_params=pltpu.CompilerParams(vmem_limit_bytes=4 << 20),
        name="finish",
    )(recv, own)


def other_core(value):
    return lax.ppermute(value, "tp", [(0, 1), (1, 0)])


def exchanged(blocks):
    return lax.all_to_all(blocks, "kv", 0, 0, tiled=True)


def body(
    tokens,
    mix_gain,
    w_query,
    w_key,
    w_value,
    w_outgate,
    w_gates,
    forget_bias,
    memory,
    normalizer,
    stabilizer,
    head_gain,
    w_out,
    mlp_gain,
    w_gate,
    w_up,
    w_down,
):
    devices = lax.axis_size("kv")
    rows, block_cols = tokens.shape
    send = project(tokens, mix_gain, w_query, w_key, w_value, w_outgate, w_gates, devices)
    heads, new_normalizer, new_stabilizer, forget, key, value_heads = state_step(
        exchanged(send),
        forget_bias,
        memory,
        normalizer,
        stabilizer,
        head_gain,
        block_cols * devices,
        w_gates.shape[1] // 2,
    )
    def behind(value):
        return lax.optimization_barrier((forget, key, value_heads, value))[:3]

    units = memory.shape[0] * memory.shape[1]
    share = units // 3
    wg, wu = w_gate.T, w_up.T
    keep, give = branch_step(exchanged(heads), w_out, wg, wu, w_down)
    part, new_normalizer, new_stabilizer = memory_step(
        memory, *behind(give), 0, share, small=(new_normalizer, new_stabilizer)
    )
    spread, own = residual_step(tokens, keep, other_core(give), part, devices)
    mine = exchanged(spread)
    part, wg, wu = memory_step(
        memory, *behind(mine), share, share, part, gain=mlp_gain[None], weights=(wg, wu)
    )
    keep, give = mixer(mine, other_core(mine), part, wg, wu, w_down)
    (new_memory,) = memory_step(memory, *behind(give), 2 * share, units - 2 * share, part)
    pair = pair_step(keep, other_core(give), new_memory)
    mixed_out = finish(exchanged(pair), own).T
    return (mixed_out, new_memory, new_normalizer, new_stabilizer.T)


def solution(mesh):
    in_specs = (
        P("dp", "kv"),
        P("kv"),
        P("kv", "tp"),
        P("kv", "tp"),
        P("kv", "tp"),
        P("kv", "tp"),
        P(),
        P("tp"),
        P(("dp", "kv"), "tp", None, None),
        P(("dp", "kv"), "tp", None),
        P(("dp", "kv"), "tp"),
        P("tp", None),
        P("tp", "kv"),
        P(),
        P(None, ("kv", "tp")),
        P(None, ("kv", "tp")),
        P(("kv", "tp"), None),
    )
    out_specs = (
        P("dp", ("kv", "tp")),
        P(("dp", "kv"), "tp", None, None),
        P(("dp", "kv"), "tp", None),
        P(("dp", "kv"), "tp"),
    )
    return jax.shard_map(body, mesh=mesh, in_specs=in_specs, out_specs=out_specs, check_vma=False)
```

```python
import jax
import jax.numpy as jnp
from jax import lax
from jax.experimental import pallas as pl
from jax.experimental.pallas import tpu as pltpu
from jax.sharding import PartitionSpec as P

QK = 128
VD = 256
EPSILON = 1e-06
LANES = 128
F32 = jnp.float32
BF16 = jnp.bfloat16
NT = (((1,), (1,)), ((), ()))
VMEM = pltpu.MemorySpace.VMEM
SMEM = pltpu.MemorySpace.SMEM
HBM = pltpu.MemorySpace.HBM


def spec(space):
    return pl.BlockSpec(memory_space=space)


def stay(*arrays):
    return [pltpu.with_memory_space_constraint(a, HBM) for a in arrays]


def fetch(pairs, sems):
    copies = [pltpu.make_async_copy(src, dst, sems.at[n]) for n, (src, dst) in enumerate(pairs)]
    for copy in copies:
        copy.start()
    return copies


def project_kernel(tokens, gain, wq, wk, wv, wo, wg, out, bt, bn, bq, bk, bv, bo, bg, sems):
    cols = tokens.shape[1]
    kv = lax.axis_index("kv")
    gate_src = wg.at[:, pl.ds(pl.multiple_of(kv * cols, LANES), cols)]
    copies = fetch(
        ((tokens, bt), (gain, bn), (wq, bq), (wk, bk), (gate_src, bg), (wv, bv), (wo, bo)), sems
    )
    blocks, rows = out.shape[:2]
    copies[0].wait()
    copies[1].wait()
    act = bt[...].astype(F32)
    square = jnp.sum(act * act, axis=1, keepdims=True)
    scaled = (act * bn[...]).astype(BF16)

    def put(value, at):
        width = value.shape[1]
        out[:, :, at : at + width] = value.reshape(blocks, rows, width).astype(BF16)

    for copy in copies[2:]:
        copy.wait()
    at = 0
    for buf in (bq, bk, bv, bo):
        put(jnp.dot(scaled, buf[...], preferred_element_type=F32), at)
        at += buf.shape[1]
    gate_count = bg.shape[0]
    wide = jnp.concatenate([bg[...].astype(F32), jnp.zeros((LANES - gate_count, cols), F32)], axis=0)
    gates = lax.dot_general(scaled, wide.astype(BF16), NT, preferred_element_type=F32)
    lane = lax.broadcasted_iota(jnp.int32, gates.shape, 1)
    put(jnp.where(lane == gate_count, square, gates), at)


def project(tokens, mix_gain, w_query, w_key, w_value, w_outgate, w_gates, blocks):
    rows, cols = tokens.shape
    width = w_query.shape[1] + w_key.shape[1] + w_value.shape[1] + w_outgate.shape[1] + LANES
    weights = (w_query, w_key, w_value, w_outgate)
    return pl.pallas_call(
        project_kernel,
        out_shape=jax.ShapeDtypeStruct((blocks, rows // blocks, width), BF16),
        in_specs=[spec(HBM)] * 7,
        out_specs=spec(VMEM),
        scratch_shapes=[pltpu.VMEM((rows, cols), BF16), pltpu.VMEM((1, cols), F32)]
        + [pltpu.VMEM(w.shape, BF16) for w in weights]
        + [pltpu.VMEM((w_gates.shape[1], cols), BF16), pltpu.SemaphoreType.DMA((7,))],
        compiler_params=pltpu.CompilerParams(vmem_limit_bytes=8 << 20),
        cost_estimate=pl.CostEstimate(flops=10**10, bytes_accessed=10**7, transcendentals=0),
        name="project",
    )(*stay(tokens, mix_gain[None], *weights, w_gates.T))


def state_kernel(
    recv, bias, memory, normalizer, stab, gain,
    heads, norm_out, stab_out, forget_out, key_out, value_out, *, model_width, total_heads,
):
    seqs, local = memory.shape[0], memory.shape[1]
    tp = lax.axis_index("tp")
    qw, vw = local * QK, local * VD

    def summed(lo, width):
        return jnp.sum(recv[:, :, lo : lo + width].astype(F32), axis=0)

    small = summed(2 * qw + 2 * vw, LANES)
    inverse = lax.rsqrt(small[:, 2 * total_heads : 2 * total_heads + 1] / model_width + EPSILON)
    query = (summed(0, qw) * inverse).astype(BF16).astype(F32)
    key = (summed(qw, qw) * (inverse * QK ** (-0.5))).astype(BF16).astype(F32)
    value = (summed(2 * qw, vw) * inverse).astype(BF16).astype(F32)
    outgate = (summed(2 * qw + vw, vw) * inverse).astype(BF16).astype(F32)
    row = lax.broadcasted_iota(jnp.int32, (seqs, QK), 0)
    diag = lax.broadcasted_iota(jnp.int32, (seqs, seqs), 0) == lax.broadcasted_iota(
        jnp.int32, (seqs, seqs), 1
    )

    def own(at, h):
        both = [small[:, at + t * local + h : at + t * local + h + 1] for t in range(total_heads // local)]
        got = both[0]
        for t in range(1, len(both)):
            got = jnp.where(tp == t, both[t], got)
        return got

    partial = []
    for h in range(local):
        input_pre = own(0, h) * inverse
        log_forget = jax.nn.log_sigmoid(own(total_heads, h) * inverse + bias[:, h : h + 1])
        old = jnp.sum(jnp.where(diag, stab[h : h + 1, :], 0.0), axis=1, keepdims=True)
        new = jnp.maximum(log_forget + old, input_pre)
        forget = jnp.exp(log_forget + old - new)
        scale = jnp.exp(input_pre - new)
        stab_out[h : h + 1, :] = jnp.sum(jnp.where(diag, new, 0.0), axis=0, keepdims=True)
        q, k = query[:, h * QK : (h + 1) * QK], key[:, h * QK : (h + 1) * QK]
        scaled_key = scale * k
        new_norm = forget * normalizer[:, h, :] + scaled_key
        norm_out[:, h, :] = new_norm
        v = value[:, h * VD : (h + 1) * VD]
        forget_out[:, h, :] = jnp.broadcast_to(forget, (seqs, LANES))
        key_out[:, h, :] = scaled_key
        value_out[:, h, :] = v
        denom = jnp.maximum(jnp.abs(jnp.sum(q * new_norm, axis=1, keepdims=True)), 1.0)
        query_key = jnp.sum(q * k, axis=1, keepdims=True)
        spread = [jnp.where(row == b, q, 0.0).astype(BF16) for b in range(seqs)]
        partial.append((forget, (scale * query_key) * v, denom, spread))
    for h in range(local):
        forget, fresh, denom, spread = partial[h]
        carried = jnp.zeros((seqs, VD), F32)
        for b in range(0, seqs, 2):
            left = jnp.concatenate([spread[b], spread[b + 1]], axis=1)
            right = jnp.concatenate([memory[b, h], memory[b + 1, h]], axis=0).astype(BF16)
            carried = carried + jnp.dot(left, right, preferred_element_type=F32)
        head_out = (forget * carried + fresh) / denom
        normed = head_out * lax.rsqrt(jnp.mean(head_out * head_out, axis=1, keepdims=True) + EPSILON)
        gate = jax.nn.sigmoid(outgate[:, h * VD : (h + 1) * VD])
        mixed = (normed * gain[h : h + 1, :] * gate).astype(BF16)
        heads[:, :, h * VD : (h + 1) * VD] = jnp.broadcast_to(mixed[None], (heads.shape[0], seqs, VD))


def state_step(recv, forget_bias, memory, normalizer, stabilizer, head_gain, model_width, total_heads):
    blocks = recv.shape[0]
    seqs, local = memory.shape[:2]

    def kernel(*refs):
        state_kernel(*refs, model_width=model_width, total_heads=total_heads)

    return pl.pallas_call(
        kernel,
        out_shape=(
            jax.ShapeDtypeStruct((blocks, seqs, local * VD), BF16),
            jax.ShapeDtypeStruct((seqs, local, QK), F32),
            jax.ShapeDtypeStruct((local, seqs), F32),
            jax.ShapeDtypeStruct((seqs, local, LANES), F32),
            jax.ShapeDtypeStruct((seqs, local, QK), F32),
            jax.ShapeDtypeStruct((seqs, local, VD), F32),
        ),
        in_specs=[spec(VMEM)] * 6,
        out_specs=[spec(VMEM)] * 6,
        compiler_params=pltpu.CompilerParams(vmem_limit_bytes=16 << 20),
        name="state",
    )(recv, forget_bias[None], memory, normalizer, stabilizer.T, head_gain)


def memory_kernel(*refs, first, count, kept, scaled):
    memory, forget, key, value = refs[:4]
    small = refs[4 : 4 + kept]
    gain, *weights = refs[4 + kept : 5 + kept + scaled] if scaled else (None,)
    outs = refs[-3 - kept - scaled : -2]
    fresh, sems = refs[-2:]
    target, small_out, scaled_out = outs[0], outs[1 : 1 + kept], outs[1 + kept :]
    seqs = memory.shape[0]
    writes = []

    def send(src, dst):
        write = pltpu.make_async_copy(src, dst, sems.at[len(writes)])
        write.start()
        writes.append(write)

    for src, dst in zip(small, small_out):
        send(src, dst)
    key_cols = {}
    for n in range(count):
        h, b = divmod(first + n, seqs)
        if h not in key_cols:
            key_cols[h] = key[:, h, :].T
        decay = forget[b : b + 1, h, :1]
        fresh[n] = decay * memory[b, h] + key_cols[h][:, b : b + 1] * value[b : b + 1, h, :]
        send(fresh.at[n], target.at[b, h])
    for src, dst in zip(weights, scaled_out):
        dst[...] = (src[...].astype(F32) * gain[...]).astype(BF16)
    for write in writes:
        write.wait()


def memory_step(memory, forget, key, value, first, count, partial=None, small=(), gain=None, weights=()):
    def kernel(*refs):
        memory_kernel(*refs, first=first, count=count, kept=len(small), scaled=len(weights))

    near = [memory, forget, key, value, *small] + ([gain, *weights] if weights else [])
    extra = [] if partial is None else stay(partial)
    outs = [HBM(memory.shape, F32)] + [HBM(a.shape, F32) for a in small]
    kinds = [spec(HBM)] * len(outs) + [spec(VMEM)] * len(weights)
    outs += [jax.ShapeDtypeStruct(w.shape, BF16) for w in weights]
    return pl.pallas_call(
        kernel,
        out_shape=outs,
        in_specs=[spec(VMEM)] * len(near) + [spec(HBM)] * len(extra),
        out_specs=kinds,
        input_output_aliases={len(near): 0} if extra else {},
        scratch_shapes=[
            pltpu.VMEM((count,) + memory.shape[2:], F32),
            pltpu.SemaphoreType.DMA((count + len(small),)),
        ],
        compiler_params=pltpu.CompilerParams(vmem_limit_bytes=6 << 20),
        cost_estimate=pl.CostEstimate(flops=0, bytes_accessed=0, transcendentals=0),
        name="memory",
    )(*near, *extra)


def mixer_kernel(mine, other, after, wg, wu, wd, keep, give, mlp):
    blocks, half, rows = mine.shape
    cols = 2 * half
    tp = lax.axis_index("tp")
    low = tp == 0
    square = jnp.zeros((half, rows), F32)
    for j in range(blocks):
        mlp[pl.ds(pl.multiple_of(j * cols + tp * half, half), half), :] = mine[j]
        mlp[pl.ds(pl.multiple_of(j * cols + (1 - tp) * half, half), half), :] = other[j]
    for j in range(blocks):
        here, there = mine[j].astype(F32), other[j].astype(F32)
        square = square + (here * here + there * there)
    inverse = lax.rsqrt(jnp.sum(square, axis=0, keepdims=True) / (blocks * cols) + EPSILON)
    gate = jnp.dot(wg[...], mlp[...], preferred_element_type=F32) * inverse
    up = jnp.dot(wu[...], mlp[...], preferred_element_type=F32) * inverse
    hidden = (jax.nn.silu(gate) * up).T.astype(BF16)
    for j in range(blocks):
        part = jnp.dot(hidden, wd[:, j * cols : (j + 1) * cols], preferred_element_type=F32).T
        first, second = part[:half].astype(BF16), part[half:].astype(BF16)
        keep[j] = jnp.where(low, first, second)
        give[j] = jnp.where(low, second, first)


def mixer(mine, other, after, gate_rows, up_rows, w_down):
    blocks, half, rows = mine.shape
    result = jax.ShapeDtypeStruct((blocks, half, rows), BF16)
    return pl.pallas_call(
        mixer_kernel,
        out_shape=(result, result),
        in_specs=[spec(VMEM)] * 2 + [spec(HBM)] + [spec(VMEM)] * 3,
        out_specs=[spec(VMEM)] * 2,
        scratch_shapes=[pltpu.VMEM((2 * blocks * half, rows), BF16)],
        compiler_params=pltpu.CompilerParams(vmem_limit_bytes=16 << 20),
        name="mixer",
    )(mine, other, *stay(after), gate_rows, up_rows, w_down)


def halves(turned):
    half = turned.shape[0] // 2
    low = lax.axis_index("tp") == 0
    first, second = turned[:half], turned[half:]
    return jnp.where(low, first, second), jnp.where(low, second, first)


def branch_kernel(heads, w_out, wg, wu, wd, keep, give):
    rows = heads[...].reshape(heads.shape[0] * heads.shape[1], w_out.shape[0])
    mine, other = halves(jnp.dot(rows, w_out[...], preferred_element_type=F32).T)
    keep[...] = mine.astype(BF16)
    give[...] = other.astype(BF16)


def branch_step(heads, w_out, *early):
    result = jax.ShapeDtypeStruct((w_out.shape[1] // 2, heads.shape[0] * heads.shape[1]), BF16)
    return pl.pallas_call(
        branch_kernel,
        out_shape=(result, result),
        in_specs=[spec(VMEM)] * (2 + len(early)),
        out_specs=[spec(VMEM)] * 2,
        compiler_params=pltpu.CompilerParams(vmem_limit_bytes=4 << 20),
        name="branch",
    )(heads, w_out, *early)


def pair_kernel(keep, got, after, out):
    out[...] = (keep[...].astype(F32) + got[...].astype(F32)).astype(BF16)


def pair_step(keep, got, after):
    return pl.pallas_call(
        pair_kernel,
        out_shape=jax.ShapeDtypeStruct(keep.shape, BF16),
        in_specs=[spec(VMEM)] * 2 + [spec(HBM)],
        out_specs=spec(VMEM),
        compiler_params=pltpu.CompilerParams(vmem_limit_bytes=4 << 20),
        name="pair",
    )(keep, got, *stay(after))


def residual_kernel(tokens, keep, got, after, spread, own):
    mine, _ = halves(tokens[...].astype(F32).T)
    rounded = (mine + (keep[...].astype(F32) + got[...].astype(F32))).astype(BF16)
    own[...] = rounded
    spread[...] = jnp.broadcast_to(rounded[None], spread.shape)


def residual_step(tokens, keep, got, after, blocks):
    return pl.pallas_call(
        residual_kernel,
        out_shape=(
            jax.ShapeDtypeStruct((blocks,) + keep.shape, BF16),
            jax.ShapeDtypeStruct(keep.shape, BF16),
        ),
        in_specs=[spec(VMEM)] * 3 + [spec(HBM)],
        out_specs=[spec(VMEM)] * 2,
        compiler_params=pltpu.CompilerParams(vmem_limit_bytes=4 << 20),
        name="residual",
    )(tokens, keep, got, *stay(after))


def finish_kernel(recv, own, out):
    out[...] = (jnp.sum(recv[...].astype(F32), axis=0) + own[...].astype(F32)).astype(BF16)


def finish(recv, own):
    return pl.pallas_call(
        finish_kernel,
        out_shape=jax.ShapeDtypeStruct(own.shape, BF16),
        in_specs=[spec(VMEM)] * 2,
        out_specs=spec(VMEM),
        compiler_params=pltpu.CompilerParams(vmem_limit_bytes=4 << 20),
        name="finish",
    )(recv, own)


def other_core(value):
    return lax.ppermute(value, "tp", [(0, 1), (1, 0)])


def exchanged(blocks):
    return lax.all_to_all(blocks, "kv", 0, 0, tiled=True)


def body(
    tokens,
    mix_gain,
    w_query,
    w_key,
    w_value,
    w_outgate,
    w_gates,
    forget_bias,
    memory,
    normalizer,
    stabilizer,
    head_gain,
    w_out,
    mlp_gain,
    w_gate,
    w_up,
    w_down,
):
    devices = lax.axis_size("kv")
    rows, block_cols = tokens.shape
    send = project(tokens, mix_gain, w_query, w_key, w_value, w_outgate, w_gates, devices)
    heads, new_normalizer, new_stabilizer, forget, key, value_heads = state_step(
        exchanged(send),
        forget_bias,
        memory,
        normalizer,
        stabilizer,
        head_gain,
        block_cols * devices,
        w_gates.shape[1] // 2,
    )
    def behind(value):
        return lax.optimization_barrier((forget, key, value_heads, value))[:3]

    units = memory.shape[0] * memory.shape[1]
    share = units // 3
    early = units // 4
    wg, wu = w_gate.T, w_up.T
    keep, give = branch_step(exchanged(heads), w_out, wg, wu, w_down)
    part, new_normalizer, new_stabilizer = memory_step(
        memory, *behind(give), 0, early, small=(new_normalizer, new_stabilizer)
    )
    spread, own = residual_step(tokens, keep, other_core(give), part, devices)
    mine = exchanged(spread)
    part, wg, wu = memory_step(
        memory, *behind(mine), early, share, part, gain=mlp_gain[None], weights=(wg, wu)
    )
    keep, give = mixer(mine, other_core(mine), part, wg, wu, w_down)
    (new_memory,) = memory_step(memory, *behind(give), early + share, units - early - share, part)
    pair = pair_step(keep, other_core(give), new_memory)
    mixed_out = finish(exchanged(pair), own).T
    return (mixed_out, new_memory, new_normalizer, new_stabilizer.T)


def solution(mesh):
    in_specs = (
        P("dp", "kv"),
        P("kv"),
        P("kv", "tp"),
        P("kv", "tp"),
        P("kv", "tp"),
        P("kv", "tp"),
        P(),
        P("tp"),
        P(("dp", "kv"), "tp", None, None),
        P(("dp", "kv"), "tp", None),
        P(("dp", "kv"), "tp"),
        P("tp", None),
        P("tp", "kv"),
        P(),
        P(None, ("kv", "tp")),
        P(None, ("kv", "tp")),
        P(("kv", "tp"), None),
    )
    out_specs = (
        P("dp", ("kv", "tp")),
        P(("dp", "kv"), "tp", None, None),
        P(("dp", "kv"), "tp", None),
        P(("dp", "kv"), "tp"),
    )
    return jax.shard_map(body, mesh=mesh, in_specs=in_specs, out_specs=out_specs, check_vma=False)
```

```python
import jax
import jax.numpy as jnp
from jax import lax
from jax.experimental import pallas as pl
from jax.experimental.pallas import tpu as pltpu
from jax.sharding import PartitionSpec as P

QK = 128
VD = 256
EPSILON = 1e-06
LANES = 128
F32 = jnp.float32
BF16 = jnp.bfloat16
NT = (((1,), (1,)), ((), ()))
VMEM = pltpu.MemorySpace.VMEM
SMEM = pltpu.MemorySpace.SMEM
HBM = pltpu.MemorySpace.HBM


def spec(space):
    return pl.BlockSpec(memory_space=space)


def stay(*arrays):
    return [pltpu.with_memory_space_constraint(a, HBM) for a in arrays]


def fetch(pairs, sems):
    copies = [pltpu.make_async_copy(src, dst, sems.at[n]) for n, (src, dst) in enumerate(pairs)]
    for copy in copies:
        copy.start()
    return copies


def project_kernel(tokens, gain, wq, wk, wv, wo, wg, out, bt, bn, bq, bk, bv, bo, bg, sems):
    cols = tokens.shape[1]
    kv = lax.axis_index("kv")
    gate_src = wg.at[:, pl.ds(pl.multiple_of(kv * cols, LANES), cols)]
    copies = fetch(
        ((tokens, bt), (gain, bn), (wq, bq), (wk, bk), (gate_src, bg), (wv, bv), (wo, bo)), sems
    )
    blocks, rows = out.shape[:2]
    copies[0].wait()
    copies[1].wait()
    act = bt[...].astype(F32)
    square = jnp.sum(act * act, axis=1, keepdims=True)
    scaled = (act * bn[...]).astype(BF16)

    def put(value, at):
        width = value.shape[1]
        out[:, :, at : at + width] = value.reshape(blocks, rows, width).astype(BF16)

    for copy in copies[2:]:
        copy.wait()
    at = 0
    for buf in (bq, bk, bv, bo):
        put(jnp.dot(scaled, buf[...], preferred_element_type=F32), at)
        at += buf.shape[1]
    gate_count = bg.shape[0]
    wide = jnp.concatenate([bg[...].astype(F32), jnp.zeros((LANES - gate_count, cols), F32)], axis=0)
    gates = lax.dot_general(scaled, wide.astype(BF16), NT, preferred_element_type=F32)
    lane = lax.broadcasted_iota(jnp.int32, gates.shape, 1)
    put(jnp.where(lane == gate_count, square, gates), at)


def project(tokens, mix_gain, w_query, w_key, w_value, w_outgate, w_gates, blocks):
    rows, cols = tokens.shape
    width = w_query.shape[1] + w_key.shape[1] + w_value.shape[1] + w_outgate.shape[1] + LANES
    weights = (w_query, w_key, w_value, w_outgate)
    return pl.pallas_call(
        project_kernel,
        out_shape=jax.ShapeDtypeStruct((blocks, rows // blocks, width), BF16),
        in_specs=[spec(HBM)] * 7,
        out_specs=spec(VMEM),
        scratch_shapes=[pltpu.VMEM((rows, cols), BF16), pltpu.VMEM((1, cols), F32)]
        + [pltpu.VMEM(w.shape, BF16) for w in weights]
        + [pltpu.VMEM((w_gates.shape[1], cols), BF16), pltpu.SemaphoreType.DMA((7,))],
        compiler_params=pltpu.CompilerParams(vmem_limit_bytes=8 << 20),
        cost_estimate=pl.CostEstimate(flops=10**10, bytes_accessed=10**7, transcendentals=0),
        name="project",
    )(*stay(tokens, mix_gain[None], *weights, w_gates.T))


def state_kernel(
    recv, bias, memory, normalizer, stab, gain,
    heads, norm_out, stab_out, forget_out, key_out, value_out, *, model_width, total_heads,
):
    seqs, local = memory.shape[0], memory.shape[1]
    tp = lax.axis_index("tp")
    qw, vw = local * QK, local * VD

    def summed(lo, width):
        return jnp.sum(recv[:, :, lo : lo + width].astype(F32), axis=0)

    small = summed(2 * qw + 2 * vw, LANES)
    inverse = lax.rsqrt(small[:, 2 * total_heads : 2 * total_heads + 1] / model_width + EPSILON)
    query = (summed(0, qw) * inverse).astype(BF16).astype(F32)
    key = (summed(qw, qw) * (inverse * QK ** (-0.5))).astype(BF16).astype(F32)
    value = (summed(2 * qw, vw) * inverse).astype(BF16).astype(F32)
    outgate = (summed(2 * qw + vw, vw) * inverse).astype(BF16).astype(F32)
    row = lax.broadcasted_iota(jnp.int32, (seqs, QK), 0)
    diag = lax.broadcasted_iota(jnp.int32, (seqs, seqs), 0) == lax.broadcasted_iota(
        jnp.int32, (seqs, seqs), 1
    )

    def own(at, h):
        both = [small[:, at + t * local + h : at + t * local + h + 1] for t in range(total_heads // local)]
        got = both[0]
        for t in range(1, len(both)):
            got = jnp.where(tp == t, both[t], got)
        return got

    partial = []
    for h in range(local):
        input_pre = own(0, h) * inverse
        log_forget = jax.nn.log_sigmoid(own(total_heads, h) * inverse + bias[:, h : h + 1])
        old = jnp.sum(jnp.where(diag, stab[h : h + 1, :], 0.0), axis=1, keepdims=True)
        new = jnp.maximum(log_forget + old, input_pre)
        forget = jnp.exp(log_forget + old - new)
        scale = jnp.exp(input_pre - new)
        stab_out[h : h + 1, :] = jnp.sum(jnp.where(diag, new, 0.0), axis=0, keepdims=True)
        q, k = query[:, h * QK : (h + 1) * QK], key[:, h * QK : (h + 1) * QK]
        scaled_key = scale * k
        new_norm = forget * normalizer[:, h, :] + scaled_key
        norm_out[:, h, :] = new_norm
        v = value[:, h * VD : (h + 1) * VD]
        forget_out[:, h, :] = jnp.broadcast_to(forget, (seqs, LANES))
        key_out[:, h, :] = scaled_key
        value_out[:, h, :] = v
        denom = jnp.maximum(jnp.abs(jnp.sum(q * new_norm, axis=1, keepdims=True)), 1.0)
        query_key = jnp.sum(q * k, axis=1, keepdims=True)
        spread = [jnp.where(row == b, q, 0.0).astype(BF16) for b in range(seqs)]
        partial.append((forget, (scale * query_key) * v, denom, spread))
    for h in range(local):
        forget, fresh, denom, spread = partial[h]
        carried = jnp.zeros((seqs, VD), F32)
        for b in range(0, seqs, 2):
            left = jnp.concatenate([spread[b], spread[b + 1]], axis=1)
            right = jnp.concatenate([memory[b, h], memory[b + 1, h]], axis=0).astype(BF16)
            carried = carried + jnp.dot(left, right, preferred_element_type=F32)
        head_out = (forget * carried + fresh) / denom
        normed = head_out * lax.rsqrt(jnp.mean(head_out * head_out, axis=1, keepdims=True) + EPSILON)
        gate = jax.nn.sigmoid(outgate[:, h * VD : (h + 1) * VD])
        mixed = (normed * gain[h : h + 1, :] * gate).astype(BF16)
        heads[:, :, h * VD : (h + 1) * VD] = jnp.broadcast_to(mixed[None], (heads.shape[0], seqs, VD))


def state_step(recv, forget_bias, memory, normalizer, stabilizer, head_gain, model_width, total_heads):
    blocks = recv.shape[0]
    seqs, local = memory.shape[:2]

    def kernel(*refs):
        state_kernel(*refs, model_width=model_width, total_heads=total_heads)

    return pl.pallas_call(
        kernel,
        out_shape=(
            jax.ShapeDtypeStruct((blocks, seqs, local * VD), BF16),
            jax.ShapeDtypeStruct((seqs, local, QK), F32),
            jax.ShapeDtypeStruct((local, seqs), F32),
            jax.ShapeDtypeStruct((seqs, local, LANES), F32),
            jax.ShapeDtypeStruct((seqs, local, QK), F32),
            jax.ShapeDtypeStruct((seqs, local, VD), F32),
        ),
        in_specs=[spec(VMEM)] * 6,
        out_specs=[spec(VMEM)] * 6,
        compiler_params=pltpu.CompilerParams(vmem_limit_bytes=16 << 20),
        name="state",
    )(recv, forget_bias[None], memory, normalizer, stabilizer.T, head_gain)


def split_job(gain, wg, wu, gate_sets, up_sets):
    half = LANES // 2
    low = lax.broadcasted_iota(jnp.int32, (wg.shape[0], LANES), 1) < half
    for src, dst in ((wg, gate_sets), (wu, up_sets)):
        for at in range(0, src.shape[1], 2 * LANES):
            one, two = (
                (src[:, lo : lo + LANES].astype(F32) * gain[:, lo : lo + LANES]).astype(BF16)
                for lo in (at, at + LANES)
            )
            first = jnp.where(low, one, pltpu.roll(two, half, 1))
            second = jnp.where(low, pltpu.roll(one, half, 1), two)
            dst[0, :, at // 2 : at // 2 + LANES] = first
            dst[1, :, at // 2 : at // 2 + LANES] = second


def partial_sums(rows_ref, gate_sets, up_sets, side):
    blocks, half, rows = rows_ref.shape
    square = jnp.zeros((half, rows), F32)
    for j in range(blocks):
        value = rows_ref[j].astype(F32)
        square = square + value * value
    flat = rows_ref[...].reshape(blocks * half, rows)
    gate = jnp.dot(gate_sets[side], flat, preferred_element_type=F32)
    up = jnp.dot(up_sets[side], flat, preferred_element_type=F32)
    return gate, up, square


def near_job(wd, mine, gate_sets, up_sets, turned, gate, up, square):
    turn_job(wd, turned)
    gate[...], up[...], square[...] = partial_sums(mine, gate_sets, up_sets, lax.axis_index("tp"))


def turn_job(wd, turned):
    cols = turned.shape[1]
    for j in range(turned.shape[0]):
        turned[j] = wd[:, j * cols : (j + 1) * cols].T


def down_half(turned, hidden, out, side):
    blocks, half, rows = out.shape
    at = pl.multiple_of(side * half, half)
    for j in range(blocks):
        part = jnp.dot(turned[j, pl.ds(at, half), :], hidden, preferred_element_type=F32)
        out[j] = part.astype(BF16)


def keep_job(turned, hidden, keep):
    down_half(turned, hidden[...], keep, lax.axis_index("tp"))


def memory_kernel(*refs, first, count, kept, job, reads):
    memory, forget, key, value = refs[:4]
    small = refs[4 : 4 + kept]
    fresh, sems = refs[-2:]
    made = len(refs) - 2 - reads[1]
    outs = refs[made - 1 - kept : made]
    target, small_out = outs[0], outs[1:]
    seqs = memory.shape[0]
    writes = []

    def send(src, dst):
        write = pltpu.make_async_copy(src, dst, sems.at[len(writes)])
        write.start()
        writes.append(write)

    for src, dst in zip(small, small_out):
        send(src, dst)
    key_cols = {}
    for n in range(count):
        h, b = divmod(first + n, seqs)
        if h not in key_cols:
            key_cols[h] = key[:, h, :].T
        decay = forget[b : b + 1, h, :1]
        fresh[n] = decay * memory[b, h] + key_cols[h][:, b : b + 1] * value[b : b + 1, h, :]
        send(fresh.at[n], target.at[b, h])
    job(*refs[4 + kept : 4 + kept + reads[0]], *refs[made:-2])
    for write in writes:
        write.wait()


def memory_step(memory, forget, key, value, first, count, job, needs, makes, partial=None, small=()):
    def kernel(*refs):
        memory_kernel(
            *refs, first=first, count=count, kept=len(small), job=job, reads=(len(needs), len(makes))
        )

    near = [memory, forget, key, value, *small, *needs]
    extra = [] if partial is None else stay(partial)
    outs = [HBM(memory.shape, F32)] + [HBM(a.shape, F32) for a in small]
    kinds = [spec(HBM)] * len(outs) + [spec(VMEM)] * len(makes)
    outs += [jax.ShapeDtypeStruct(shape, kind) for shape, kind in makes]
    return pl.pallas_call(
        kernel,
        out_shape=outs,
        in_specs=[spec(VMEM)] * len(near) + [spec(HBM)] * len(extra),
        out_specs=kinds,
        input_output_aliases={len(near): 0} if extra else {},
        scratch_shapes=[
            pltpu.VMEM((count,) + memory.shape[2:], F32),
            pltpu.SemaphoreType.DMA((count + len(small),)),
        ],
        compiler_params=pltpu.CompilerParams(vmem_limit_bytes=8 << 20),
        cost_estimate=pl.CostEstimate(flops=0, bytes_accessed=0, transcendentals=0),
        name="memory",
    )(*near, *extra)


def mixer_kernel(other, after, near_gate, near_up, near_square, gate_sets, up_sets, turned, give, hidden):
    blocks, half, _ = other.shape
    tp = lax.axis_index("tp")
    gate, up, square = partial_sums(other, gate_sets, up_sets, 1 - tp)
    square = jnp.sum(square + near_square[...], axis=0, keepdims=True)
    inverse = lax.rsqrt(square / (2 * blocks * half) + EPSILON)
    gate = (gate + near_gate[...]) * inverse
    up = (up + near_up[...]) * inverse
    value = (jax.nn.silu(gate) * up).astype(BF16)
    hidden[...] = value
    down_half(turned, value, give, 1 - tp)


def mixer(other, after, *near):
    blocks, half, rows = other.shape
    return pl.pallas_call(
        mixer_kernel,
        out_shape=(
            jax.ShapeDtypeStruct((blocks, half, rows), BF16),
            jax.ShapeDtypeStruct(near[0].shape, BF16),
        ),
        in_specs=[spec(VMEM), spec(HBM)] + [spec(VMEM)] * len(near),
        out_specs=[spec(VMEM)] * 2,
        compiler_params=pltpu.CompilerParams(vmem_limit_bytes=8 << 20),
        name="mixer",
    )(other, *stay(after), *near)


def halves(turned):
    half = turned.shape[0] // 2
    low = lax.axis_index("tp") == 0
    first, second = turned[:half], turned[half:]
    return jnp.where(low, first, second), jnp.where(low, second, first)


def branch_kernel(heads, w_out, wg, wu, wd, keep, give):
    rows = heads[...].reshape(heads.shape[0] * heads.shape[1], w_out.shape[0])
    mine, other = halves(jnp.dot(rows, w_out[...], preferred_element_type=F32).T)
    keep[...] = mine.astype(BF16)
    give[...] = other.astype(BF16)


def branch_step(heads, w_out, *early):
    result = jax.ShapeDtypeStruct((w_out.shape[1] // 2, heads.shape[0] * heads.shape[1]), BF16)
    return pl.pallas_call(
        branch_kernel,
        out_shape=(result, result),
        in_specs=[spec(VMEM)] * (2 + len(early)),
        out_specs=[spec(VMEM)] * 2,
        compiler_params=pltpu.CompilerParams(vmem_limit_bytes=4 << 20),
        name="branch",
    )(heads, w_out, *early)


def pair_kernel(keep, got, after, out):
    out[...] = (keep[...].astype(F32) + got[...].astype(F32)).astype(BF16)


def pair_step(keep, got, after):
    return pl.pallas_call(
        pair_kernel,
        out_shape=jax.ShapeDtypeStruct(keep.shape, BF16),
        in_specs=[spec(VMEM)] * 2 + [spec(HBM)],
        out_specs=spec(VMEM),
        compiler_params=pltpu.CompilerParams(vmem_limit_bytes=4 << 20),
        name="pair",
    )(keep, got, *stay(after))


def residual_kernel(tokens, keep, got, after, spread, own):
    mine, _ = halves(tokens[...].astype(F32).T)
    rounded = (mine + (keep[...].astype(F32) + got[...].astype(F32))).astype(BF16)
    own[...] = rounded
    spread[...] = jnp.broadcast_to(rounded[None], spread.shape)


def residual_step(tokens, keep, got, after, blocks):
    return pl.pallas_call(
        residual_kernel,
        out_shape=(
            jax.ShapeDtypeStruct((blocks,) + keep.shape, BF16),
            jax.ShapeDtypeStruct(keep.shape, BF16),
        ),
        in_specs=[spec(VMEM)] * 3 + [spec(HBM)],
        out_specs=[spec(VMEM)] * 2,
        compiler_params=pltpu.CompilerParams(vmem_limit_bytes=4 << 20),
        name="residual",
    )(tokens, keep, got, *stay(after))


def finish_kernel(recv, own, out):
    out[...] = (jnp.sum(recv[...].astype(F32), axis=0) + own[...].astype(F32)).astype(BF16)


def finish(recv, own):
    return pl.pallas_call(
        finish_kernel,
        out_shape=jax.ShapeDtypeStruct(own.shape, BF16),
        in_specs=[spec(VMEM)] * 2,
        out_specs=spec(VMEM),
        compiler_params=pltpu.CompilerParams(vmem_limit_bytes=4 << 20),
        name="finish",
    )(recv, own)


def other_core(value):
    return lax.ppermute(value, "tp", [(0, 1), (1, 0)])


def exchanged(blocks):
    return lax.all_to_all(blocks, "kv", 0, 0, tiled=True)


def body(
    tokens,
    mix_gain,
    w_query,
    w_key,
    w_value,
    w_outgate,
    w_gates,
    forget_bias,
    memory,
    normalizer,
    stabilizer,
    head_gain,
    w_out,
    mlp_gain,
    w_gate,
    w_up,
    w_down,
):
    devices = lax.axis_size("kv")
    rows, block_cols = tokens.shape
    send = project(tokens, mix_gain, w_query, w_key, w_value, w_outgate, w_gates, devices)
    heads, new_normalizer, new_stabilizer, forget, key, value_heads = state_step(
        exchanged(send),
        forget_bias,
        memory,
        normalizer,
        stabilizer,
        head_gain,
        block_cols * devices,
        w_gates.shape[1] // 2,
    )
    def behind(value):
        return lax.optimization_barrier((forget, key, value_heads, value))[:3]

    units = memory.shape[0] * memory.shape[1]
    early, share = 3 * units // 16, 11 * units // 32
    wg, wu = w_gate.T, w_up.T
    keep, give = branch_step(exchanged(heads), w_out, wg, wu, w_down)
    sets = (2, wg.shape[0], wg.shape[1] // 2)
    part, new_normalizer, new_stabilizer, gate_sets, up_sets = memory_step(
        memory, *behind(give), 0, early, split_job, (mlp_gain[None], wg, wu),
        ((sets, BF16), (sets, BF16)), small=(new_normalizer, new_stabilizer),
    )
    spread, own = residual_step(tokens, keep, other_core(give), part, devices)
    mine = exchanged(spread)
    hidden_shape = (wg.shape[0], rows)
    part, turned, *near = memory_step(
        memory, *behind(mine), early, share, near_job, (w_down, mine, gate_sets, up_sets),
        (((devices, block_cols, w_down.shape[0]), BF16), (hidden_shape, F32), (hidden_shape, F32), (own.shape, F32)),
        part,
    )
    give, hidden = mixer(other_core(mine), part, *near, gate_sets, up_sets, turned)
    new_memory, keep = memory_step(
        memory, *behind(give), early + share, units - early - share, keep_job, (turned, hidden),
        ((give.shape, BF16),), part,
    )
    pair = pair_step(keep, other_core(give), new_memory)
    mixed_out = finish(exchanged(pair), own).T
    return (mixed_out, new_memory, new_normalizer, new_stabilizer.T)


def solution(mesh):
    in_specs = (
        P("dp", "kv"),
        P("kv"),
        P("kv", "tp"),
        P("kv", "tp"),
        P("kv", "tp"),
        P("kv", "tp"),
        P(),
        P("tp"),
        P(("dp", "kv"), "tp", None, None),
        P(("dp", "kv"), "tp", None),
        P(("dp", "kv"), "tp"),
        P("tp", None),
        P("tp", "kv"),
        P(),
        P(None, ("kv", "tp")),
        P(None, ("kv", "tp")),
        P(("kv", "tp"), None),
    )
    out_specs = (
        P("dp", ("kv", "tp")),
        P(("dp", "kv"), "tp", None, None),
        P(("dp", "kv"), "tp", None),
        P(("dp", "kv"), "tp"),
    )
    return jax.shard_map(body, mesh=mesh, in_specs=in_specs, out_specs=out_specs, check_vma=False)
```

```python
import jax
import jax.numpy as jnp
from jax import lax
from jax.experimental import pallas as pl
from jax.experimental.pallas import tpu as pltpu
from jax.sharding import PartitionSpec as P

QK = 128
VD = 256
EPSILON = 1e-06
LANES = 128
F32 = jnp.float32
BF16 = jnp.bfloat16
NT = (((1,), (1,)), ((), ()))
VMEM = pltpu.MemorySpace.VMEM
SMEM = pltpu.MemorySpace.SMEM
HBM = pltpu.MemorySpace.HBM


def spec(space):
    return pl.BlockSpec(memory_space=space)


def stay(*arrays):
    return [pltpu.with_memory_space_constraint(a, HBM) for a in arrays]


def fetch(pairs, sems):
    copies = [pltpu.make_async_copy(src, dst, sems.at[n]) for n, (src, dst) in enumerate(pairs)]
    for copy in copies:
        copy.start()
    return copies


def project_kernel(tokens, gain, wq, wk, wv, wo, wg, out, bt, bn, bq, bk, bv, bo, bg, sems):
    cols = tokens.shape[1]
    kv = lax.axis_index("kv")
    gate_src = wg.at[:, pl.ds(pl.multiple_of(kv * cols, LANES), cols)]
    copies = fetch(
        ((tokens, bt), (gain, bn), (wq, bq), (wk, bk), (gate_src, bg), (wv, bv), (wo, bo)), sems
    )
    blocks, rows = out.shape[:2]
    copies[0].wait()
    copies[1].wait()
    act = bt[...].astype(F32)
    square = jnp.sum(act * act, axis=1, keepdims=True)
    scaled = (act * bn[...]).astype(BF16)

    def put(value, at):
        width = value.shape[1]
        out[:, :, at : at + width] = value.reshape(blocks, rows, width).astype(BF16)

    for copy in copies[2:]:
        copy.wait()
    at = 0
    for buf in (bq, bk, bv, bo):
        put(jnp.dot(scaled, buf[...], preferred_element_type=F32), at)
        at += buf.shape[1]
    gate_count = bg.shape[0]
    wide = jnp.concatenate([bg[...].astype(F32), jnp.zeros((LANES - gate_count, cols), F32)], axis=0)
    gates = lax.dot_general(scaled, wide.astype(BF16), NT, preferred_element_type=F32)
    lane = lax.broadcasted_iota(jnp.int32, gates.shape, 1)
    put(jnp.where(lane == gate_count, square, gates), at)


def project(tokens, mix_gain, w_query, w_key, w_value, w_outgate, w_gates, blocks):
    rows, cols = tokens.shape
    width = w_query.shape[1] + w_key.shape[1] + w_value.shape[1] + w_outgate.shape[1] + LANES
    weights = (w_query, w_key, w_value, w_outgate)
    return pl.pallas_call(
        project_kernel,
        out_shape=jax.ShapeDtypeStruct((blocks, rows // blocks, width), BF16),
        in_specs=[spec(HBM)] * 7,
        out_specs=spec(VMEM),
        scratch_shapes=[pltpu.VMEM((rows, cols), BF16), pltpu.VMEM((1, cols), F32)]
        + [pltpu.VMEM(w.shape, BF16) for w in weights]
        + [pltpu.VMEM((w_gates.shape[1], cols), BF16), pltpu.SemaphoreType.DMA((7,))],
        compiler_params=pltpu.CompilerParams(vmem_limit_bytes=8 << 20),
        cost_estimate=pl.CostEstimate(flops=10**10, bytes_accessed=10**7, transcendentals=0),
        name="project",
    )(*stay(tokens, mix_gain[None], *weights, w_gates.T))


def state_kernel(
    recv, bias, memory, normalizer, stab, gain,
    heads, norm_out, stab_out, forget_out, key_out, value_out, *, model_width, total_heads,
):
    seqs, local = memory.shape[0], memory.shape[1]
    tp = lax.axis_index("tp")
    qw, vw = local * QK, local * VD

    def summed(lo, width):
        return jnp.sum(recv[:, :, lo : lo + width].astype(F32), axis=0)

    small = summed(2 * qw + 2 * vw, LANES)
    inverse = lax.rsqrt(small[:, 2 * total_heads : 2 * total_heads + 1] / model_width + EPSILON)
    query = (summed(0, qw) * inverse).astype(BF16).astype(F32)
    key = (summed(qw, qw) * (inverse * QK ** (-0.5))).astype(BF16).astype(F32)
    value = (summed(2 * qw, vw) * inverse).astype(BF16).astype(F32)
    outgate = (summed(2 * qw + vw, vw) * inverse).astype(BF16).astype(F32)
    row = lax.broadcasted_iota(jnp.int32, (seqs, QK), 0)
    diag = lax.broadcasted_iota(jnp.int32, (seqs, seqs), 0) == lax.broadcasted_iota(
        jnp.int32, (seqs, seqs), 1
    )

    def own(at, h):
        both = [small[:, at + t * local + h : at + t * local + h + 1] for t in range(total_heads // local)]
        got = both[0]
        for t in range(1, len(both)):
            got = jnp.where(tp == t, both[t], got)
        return got

    partial = []
    for h in range(local):
        input_pre = own(0, h) * inverse
        log_forget = jax.nn.log_sigmoid(own(total_heads, h) * inverse + bias[:, h : h + 1])
        old = jnp.sum(jnp.where(diag, stab[h : h + 1, :], 0.0), axis=1, keepdims=True)
        new = jnp.maximum(log_forget + old, input_pre)
        forget = jnp.exp(log_forget + old - new)
        scale = jnp.exp(input_pre - new)
        stab_out[h : h + 1, :] = jnp.sum(jnp.where(diag, new, 0.0), axis=0, keepdims=True)
        q, k = query[:, h * QK : (h + 1) * QK], key[:, h * QK : (h + 1) * QK]
        scaled_key = scale * k
        new_norm = forget * normalizer[:, h, :] + scaled_key
        norm_out[:, h, :] = new_norm
        v = value[:, h * VD : (h + 1) * VD]
        forget_out[:, h, :] = jnp.broadcast_to(forget, (seqs, LANES))
        key_out[:, h, :] = scaled_key
        value_out[:, h, :] = v
        denom = jnp.maximum(jnp.abs(jnp.sum(q * new_norm, axis=1, keepdims=True)), 1.0)
        query_key = jnp.sum(q * k, axis=1, keepdims=True)
        spread = [jnp.where(row == b, q, 0.0).astype(BF16) for b in range(seqs)]
        partial.append((forget, (scale * query_key) * v, denom, spread))
    for h in range(local):
        forget, fresh, denom, spread = partial[h]
        carried = jnp.zeros((seqs, VD), F32)
        for b in range(0, seqs, 2):
            left = jnp.concatenate([spread[b], spread[b + 1]], axis=1)
            right = jnp.concatenate([memory[b, h], memory[b + 1, h]], axis=0).astype(BF16)
            carried = carried + jnp.dot(left, right, preferred_element_type=F32)
        head_out = (forget * carried + fresh) / denom
        normed = head_out * lax.rsqrt(jnp.mean(head_out * head_out, axis=1, keepdims=True) + EPSILON)
        gate = jax.nn.sigmoid(outgate[:, h * VD : (h + 1) * VD])
        mixed = (normed * gain[h : h + 1, :] * gate).astype(BF16)
        heads[:, :, h * VD : (h + 1) * VD] = jnp.broadcast_to(mixed[None], (heads.shape[0], seqs, VD))


def state_step(recv, forget_bias, memory, normalizer, stabilizer, head_gain, model_width, total_heads):
    blocks = recv.shape[0]
    seqs, local = memory.shape[:2]

    def kernel(*refs):
        state_kernel(*refs, model_width=model_width, total_heads=total_heads)

    return pl.pallas_call(
        kernel,
        out_shape=(
            jax.ShapeDtypeStruct((blocks, seqs, local * VD), BF16),
            jax.ShapeDtypeStruct((seqs, local, QK), F32),
            jax.ShapeDtypeStruct((local, seqs), F32),
            jax.ShapeDtypeStruct((seqs, local, LANES), F32),
            jax.ShapeDtypeStruct((seqs, local, QK), F32),
            jax.ShapeDtypeStruct((seqs, local, VD), F32),
        ),
        in_specs=[spec(VMEM)] * 6,
        out_specs=[spec(VMEM)] * 6,
        compiler_params=pltpu.CompilerParams(vmem_limit_bytes=16 << 20),
        name="state",
    )(recv, forget_bias[None], memory, normalizer, stabilizer.T, head_gain)


def split_job(gain, wg, wu, gate_sets, up_sets):
    half = LANES // 2
    low = lax.broadcasted_iota(jnp.int32, (wg.shape[0], LANES), 1) < half
    for src, dst in ((wg, gate_sets), (wu, up_sets)):
        for at in range(0, src.shape[1], 2 * LANES):
            one, two = (
                (src[:, lo : lo + LANES].astype(F32) * gain[:, lo : lo + LANES]).astype(BF16)
                for lo in (at, at + LANES)
            )
            first = jnp.where(low, one, pltpu.roll(two, half, 1))
            second = jnp.where(low, pltpu.roll(one, half, 1), two)
            dst[0, :, at // 2 : at // 2 + LANES] = first
            dst[1, :, at // 2 : at // 2 + LANES] = second


def partial_sums(rows_ref, gate_sets, up_sets, side):
    blocks, half, rows = rows_ref.shape
    square = jnp.zeros((half, rows), F32)
    for j in range(blocks):
        value = rows_ref[j].astype(F32)
        square = square + value * value
    flat = rows_ref[...].reshape(blocks * half, rows)
    gate = jnp.dot(gate_sets[side], flat, preferred_element_type=F32)
    up = jnp.dot(up_sets[side], flat, preferred_element_type=F32)
    return gate, up, square


def near_job(wd, mine, gate_sets, up_sets, turned, gate, up, square):
    turn_job(wd, turned)
    gate[...], up[...], square[...] = partial_sums(mine, gate_sets, up_sets, lax.axis_index("tp"))


def turn_job(wd, turned):
    cols = turned.shape[1]
    for j in range(turned.shape[0]):
        turned[j] = wd[:, j * cols : (j + 1) * cols].T


def down_half(turned, hidden, out, side):
    blocks, half, rows = out.shape
    at = pl.multiple_of(side * half, half)
    for j in range(blocks):
        part = jnp.dot(turned[j, pl.ds(at, half), :], hidden, preferred_element_type=F32)
        out[j] = part.astype(BF16)


def keep_job(turned, hidden, keep):
    down_half(turned, hidden[...], keep, lax.axis_index("tp"))


def memory_kernel(*refs, first, count, kept, job, reads):
    memory, forget, key, value = refs[:4]
    small = refs[4 : 4 + kept]
    fresh, sems = refs[-2:]
    made = len(refs) - 2 - reads[1]
    outs = refs[made - 1 - kept : made]
    target, small_out = outs[0], outs[1:]
    seqs = memory.shape[0]
    writes = []

    def send(src, dst):
        write = pltpu.make_async_copy(src, dst, sems.at[len(writes)])
        write.start()
        writes.append(write)

    for src, dst in zip(small, small_out):
        send(src, dst)
    key_cols = {}
    for n in range(count):
        h, b = divmod(first + n, seqs)
        if h not in key_cols:
            key_cols[h] = key[:, h, :].T
        decay = forget[b : b + 1, h, :1]
        fresh[n] = decay * memory[b, h] + key_cols[h][:, b : b + 1] * value[b : b + 1, h, :]
        send(fresh.at[n], target.at[b, h])
    job(*refs[4 + kept : 4 + kept + reads[0]], *refs[made:-2])
    for write in writes:
        write.wait()


def memory_step(memory, forget, key, value, first, count, job, needs, makes, partial=None, small=()):
    def kernel(*refs):
        memory_kernel(
            *refs, first=first, count=count, kept=len(small), job=job, reads=(len(needs), len(makes))
        )

    near = [memory, forget, key, value, *small, *needs]
    extra = [] if partial is None else stay(partial)
    outs = [HBM(memory.shape, F32)] + [HBM(a.shape, F32) for a in small]
    kinds = [spec(HBM)] * len(outs) + [spec(VMEM)] * len(makes)
    outs += [jax.ShapeDtypeStruct(shape, kind) for shape, kind in makes]
    return pl.pallas_call(
        kernel,
        out_shape=outs,
        in_specs=[spec(VMEM)] * len(near) + [spec(HBM)] * len(extra),
        out_specs=kinds,
        input_output_aliases={len(near): 0} if extra else {},
        scratch_shapes=[
            pltpu.VMEM((count,) + memory.shape[2:], F32),
            pltpu.SemaphoreType.DMA((count + len(small),)),
        ],
        compiler_params=pltpu.CompilerParams(vmem_limit_bytes=8 << 20),
        cost_estimate=pl.CostEstimate(flops=0, bytes_accessed=0, transcendentals=0),
        name="memory",
    )(*near, *extra)


def mixer_kernel(other, after, near_gate, near_up, near_square, gate_sets, up_sets, turned, give, hidden):
    blocks, half, _ = other.shape
    tp = lax.axis_index("tp")
    gate, up, square = partial_sums(other, gate_sets, up_sets, 1 - tp)
    square = jnp.sum(square + near_square[...], axis=0, keepdims=True)
    inverse = lax.rsqrt(square / (2 * blocks * half) + EPSILON)
    gate = (gate + near_gate[...]) * inverse
    up = (up + near_up[...]) * inverse
    value = (jax.nn.silu(gate) * up).astype(BF16)
    hidden[...] = value
    down_half(turned, value, give, 1 - tp)


def mixer(other, after, *near):
    blocks, half, rows = other.shape
    return pl.pallas_call(
        mixer_kernel,
        out_shape=(
            jax.ShapeDtypeStruct((blocks, half, rows), BF16),
            jax.ShapeDtypeStruct(near[0].shape, BF16),
        ),
        in_specs=[spec(VMEM), spec(HBM)] + [spec(VMEM)] * len(near),
        out_specs=[spec(VMEM)] * 2,
        compiler_params=pltpu.CompilerParams(vmem_limit_bytes=8 << 20),
        name="mixer",
    )(other, *stay(after), *near)


def halves(turned):
    half = turned.shape[0] // 2
    low = lax.axis_index("tp") == 0
    first, second = turned[:half], turned[half:]
    return jnp.where(low, first, second), jnp.where(low, second, first)


def branch_kernel(heads, w_out, wg, wu, wd, keep, give):
    rows = heads[...].reshape(heads.shape[0] * heads.shape[1], w_out.shape[0])
    mine, other = halves(jnp.dot(rows, w_out[...], preferred_element_type=F32).T)
    keep[...] = mine.astype(BF16)
    give[...] = other.astype(BF16)


def branch_step(heads, w_out, *early):
    result = jax.ShapeDtypeStruct((w_out.shape[1] // 2, heads.shape[0] * heads.shape[1]), BF16)
    return pl.pallas_call(
        branch_kernel,
        out_shape=(result, result),
        in_specs=[spec(VMEM)] * (2 + len(early)),
        out_specs=[spec(VMEM)] * 2,
        compiler_params=pltpu.CompilerParams(vmem_limit_bytes=4 << 20),
        name="branch",
    )(heads, w_out, *early)


def pair_kernel(keep, got, after, out):
    out[...] = (keep[...].astype(F32) + got[...].astype(F32)).astype(BF16)


def pair_step(keep, got, after):
    return pl.pallas_call(
        pair_kernel,
        out_shape=jax.ShapeDtypeStruct(keep.shape, BF16),
        in_specs=[spec(VMEM)] * 2 + [spec(HBM)],
        out_specs=spec(VMEM),
        compiler_params=pltpu.CompilerParams(vmem_limit_bytes=4 << 20),
        name="pair",
    )(keep, got, *stay(after))


def residual_kernel(tokens, keep, got, after, spread, own):
    mine, _ = halves(tokens[...].astype(F32).T)
    rounded = (mine + (keep[...].astype(F32) + got[...].astype(F32))).astype(BF16)
    own[...] = rounded
    spread[...] = jnp.broadcast_to(rounded[None], spread.shape)


def residual_step(tokens, keep, got, after, blocks):
    return pl.pallas_call(
        residual_kernel,
        out_shape=(
            jax.ShapeDtypeStruct((blocks,) + keep.shape, BF16),
            jax.ShapeDtypeStruct(keep.shape, BF16),
        ),
        in_specs=[spec(VMEM)] * 3 + [spec(HBM)],
        out_specs=[spec(VMEM)] * 2,
        compiler_params=pltpu.CompilerParams(vmem_limit_bytes=4 << 20),
        name="residual",
    )(tokens, keep, got, *stay(after))


def finish_kernel(recv, own, out):
    out[...] = (jnp.sum(recv[...].astype(F32), axis=0) + own[...].astype(F32)).astype(BF16)


def finish(recv, own):
    return pl.pallas_call(
        finish_kernel,
        out_shape=jax.ShapeDtypeStruct(own.shape, BF16),
        in_specs=[spec(VMEM)] * 2,
        out_specs=spec(VMEM),
        compiler_params=pltpu.CompilerParams(vmem_limit_bytes=4 << 20),
        name="finish",
    )(recv, own)


def other_core(value):
    return lax.ppermute(value, "tp", [(0, 1), (1, 0)])


def exchanged(blocks):
    return lax.all_to_all(blocks, "kv", 0, 0, tiled=True)


def body(
    tokens,
    mix_gain,
    w_query,
    w_key,
    w_value,
    w_outgate,
    w_gates,
    forget_bias,
    memory,
    normalizer,
    stabilizer,
    head_gain,
    w_out,
    mlp_gain,
    w_gate,
    w_up,
    w_down,
):
    devices = lax.axis_size("kv")
    rows, block_cols = tokens.shape
    send = project(tokens, mix_gain, w_query, w_key, w_value, w_outgate, w_gates, devices)
    heads, new_normalizer, new_stabilizer, forget, key, value_heads = state_step(
        exchanged(send),
        forget_bias,
        memory,
        normalizer,
        stabilizer,
        head_gain,
        block_cols * devices,
        w_gates.shape[1] // 2,
    )
    def behind(value):
        return lax.optimization_barrier((forget, key, value_heads, value))[:3]

    units = memory.shape[0] * memory.shape[1]
    early, share = 7 * units // 32, 11 * units // 32
    wg, wu = w_gate.T, w_up.T
    keep, give = branch_step(exchanged(heads), w_out, wg, wu, w_down)
    sets = (2, wg.shape[0], wg.shape[1] // 2)
    part, new_normalizer, new_stabilizer, gate_sets, up_sets = memory_step(
        memory, *behind(give), 0, early, split_job, (mlp_gain[None], wg, wu),
        ((sets, BF16), (sets, BF16)), small=(new_normalizer, new_stabilizer),
    )
    spread, own = residual_step(tokens, keep, other_core(give), part, devices)
    mine = exchanged(spread)
    hidden_shape = (wg.shape[0], rows)
    part, turned, *near = memory_step(
        memory, *behind(mine), early, share, near_job, (w_down, mine, gate_sets, up_sets),
        (((devices, block_cols, w_down.shape[0]), BF16), (hidden_shape, F32), (hidden_shape, F32), (own.shape, F32)),
        part,
    )
    give, hidden = mixer(other_core(mine), part, *near, gate_sets, up_sets, turned)
    new_memory, keep = memory_step(
        memory, *behind(give), early + share, units - early - share, keep_job, (turned, hidden),
        ((give.shape, BF16),), part,
    )
    pair = pair_step(keep, other_core(give), new_memory)
    mixed_out = finish(exchanged(pair), own).T
    return (mixed_out, new_memory, new_normalizer, new_stabilizer.T)


def solution(mesh):
    in_specs = (
        P("dp", "kv"),
        P("kv"),
        P("kv", "tp"),
        P("kv", "tp"),
        P("kv", "tp"),
        P("kv", "tp"),
        P(),
        P("tp"),
        P(("dp", "kv"), "tp", None, None),
        P(("dp", "kv"), "tp", None),
        P(("dp", "kv"), "tp"),
        P("tp", None),
        P("tp", "kv"),
        P(),
        P(None, ("kv", "tp")),
        P(None, ("kv", "tp")),
        P(("kv", "tp"), None),
    )
    out_specs = (
        P("dp", ("kv", "tp")),
        P(("dp", "kv"), "tp", None, None),
        P(("dp", "kv"), "tp", None),
        P(("dp", "kv"), "tp"),
    )
    return jax.shard_map(body, mesh=mesh, in_specs=in_specs, out_specs=out_specs, check_vma=False)
```

```python
import jax
import jax.numpy as jnp
from jax import lax
from jax.experimental import pallas as pl
from jax.experimental.pallas import tpu as pltpu
from jax.sharding import PartitionSpec as P

QK = 128
VD = 256
EPSILON = 1e-06
LANES = 128
F32 = jnp.float32
BF16 = jnp.bfloat16
NT = (((1,), (1,)), ((), ()))
VMEM = pltpu.MemorySpace.VMEM
SMEM = pltpu.MemorySpace.SMEM
HBM = pltpu.MemorySpace.HBM


def spec(space):
    return pl.BlockSpec(memory_space=space)


def stay(*arrays):
    return [pltpu.with_memory_space_constraint(a, HBM) for a in arrays]


def fetch(pairs, sems):
    copies = [pltpu.make_async_copy(src, dst, sems.at[n]) for n, (src, dst) in enumerate(pairs)]
    for copy in copies:
        copy.start()
    return copies


def project_kernel(tokens, gain, wq, wk, wv, wo, wg, out, bt, bn, bq, bk, bv, bo, bg, sems):
    cols = tokens.shape[1]
    kv = lax.axis_index("kv")
    gate_src = wg.at[:, pl.ds(pl.multiple_of(kv * cols, LANES), cols)]
    copies = fetch(
        ((tokens, bt), (gain, bn), (wq, bq), (wk, bk), (gate_src, bg), (wv, bv), (wo, bo)), sems
    )
    blocks, rows = out.shape[:2]
    copies[0].wait()
    copies[1].wait()
    act = bt[...].astype(F32)
    square = jnp.sum(act * act, axis=1, keepdims=True)
    scaled = (act * bn[...]).astype(BF16)

    def put(value, at):
        width = value.shape[1]
        out[:, :, at : at + width] = value.reshape(blocks, rows, width).astype(BF16)

    for copy in copies[2:]:
        copy.wait()
    at = 0
    for buf in (bq, bk, bv, bo):
        put(jnp.dot(scaled, buf[...], preferred_element_type=F32), at)
        at += buf.shape[1]
    gate_count = bg.shape[0]
    wide = jnp.concatenate([bg[...].astype(F32), jnp.zeros((LANES - gate_count, cols), F32)], axis=0)
    gates = lax.dot_general(scaled, wide.astype(BF16), NT, preferred_element_type=F32)
    lane = lax.broadcasted_iota(jnp.int32, gates.shape, 1)
    put(jnp.where(lane == gate_count, square, gates), at)


def project(tokens, mix_gain, w_query, w_key, w_value, w_outgate, w_gates, blocks):
    rows, cols = tokens.shape
    width = w_query.shape[1] + w_key.shape[1] + w_value.shape[1] + w_outgate.shape[1] + LANES
    weights = (w_query, w_key, w_value, w_outgate)
    return pl.pallas_call(
        project_kernel,
        out_shape=jax.ShapeDtypeStruct((blocks, rows // blocks, width), BF16),
        in_specs=[spec(HBM)] * 7,
        out_specs=spec(VMEM),
        scratch_shapes=[pltpu.VMEM((rows, cols), BF16), pltpu.VMEM((1, cols), F32)]
        + [pltpu.VMEM(w.shape, BF16) for w in weights]
        + [pltpu.VMEM((w_gates.shape[1], cols), BF16), pltpu.SemaphoreType.DMA((7,))],
        compiler_params=pltpu.CompilerParams(vmem_limit_bytes=8 << 20),
        cost_estimate=pl.CostEstimate(flops=10**10, bytes_accessed=10**7, transcendentals=0),
        name="project",
    )(*stay(tokens, mix_gain[None], *weights, w_gates.T))


def state_kernel(
    recv, bias, memory, normalizer, stab, gain,
    heads, norm_out, stab_out, forget_out, key_out, value_out, *, model_width, total_heads,
):
    seqs, local = memory.shape[0], memory.shape[1]
    tp = lax.axis_index("tp")
    qw, vw = local * QK, local * VD

    def summed(lo, width):
        return jnp.sum(recv[:, :, lo : lo + width].astype(F32), axis=0)

    small = summed(2 * qw + 2 * vw, LANES)
    inverse = lax.rsqrt(small[:, 2 * total_heads : 2 * total_heads + 1] / model_width + EPSILON)
    query = (summed(0, qw) * inverse).astype(BF16).astype(F32)
    key = (summed(qw, qw) * (inverse * QK ** (-0.5))).astype(BF16).astype(F32)
    value = (summed(2 * qw, vw) * inverse).astype(BF16).astype(F32)
    outgate = (summed(2 * qw + vw, vw) * inverse).astype(BF16).astype(F32)
    row = lax.broadcasted_iota(jnp.int32, (seqs, QK), 0)
    diag = lax.broadcasted_iota(jnp.int32, (seqs, seqs), 0) == lax.broadcasted_iota(
        jnp.int32, (seqs, seqs), 1
    )

    def own(at, h):
        both = [small[:, at + t * local + h : at + t * local + h + 1] for t in range(total_heads // local)]
        got = both[0]
        for t in range(1, len(both)):
            got = jnp.where(tp == t, both[t], got)
        return got

    partial = []
    for h in range(local):
        input_pre = own(0, h) * inverse
        log_forget = jax.nn.log_sigmoid(own(total_heads, h) * inverse + bias[:, h : h + 1])
        old = jnp.sum(jnp.where(diag, stab[h : h + 1, :], 0.0), axis=1, keepdims=True)
        new = jnp.maximum(log_forget + old, input_pre)
        forget = jnp.exp(log_forget + old - new)
        scale = jnp.exp(input_pre - new)
        stab_out[h : h + 1, :] = jnp.sum(jnp.where(diag, new, 0.0), axis=0, keepdims=True)
        q, k = query[:, h * QK : (h + 1) * QK], key[:, h * QK : (h + 1) * QK]
        scaled_key = scale * k
        new_norm = forget * normalizer[:, h, :] + scaled_key
        norm_out[:, h, :] = new_norm
        v = value[:, h * VD : (h + 1) * VD]
        forget_out[:, h, :] = jnp.broadcast_to(forget, (seqs, LANES))
        key_out[:, h, :] = scaled_key
        value_out[:, h, :] = v
        denom = jnp.maximum(jnp.abs(jnp.sum(q * new_norm, axis=1, keepdims=True)), 1.0)
        query_key = jnp.sum(q * k, axis=1, keepdims=True)
        spread = [jnp.where(row == b, q, 0.0).astype(BF16) for b in range(seqs)]
        partial.append((forget, (scale * query_key) * v, denom, spread))
    for h in range(local):
        forget, fresh, denom, spread = partial[h]
        carried = jnp.zeros((seqs, VD), F32)
        for b in range(0, seqs, 2):
            left = jnp.concatenate([spread[b], spread[b + 1]], axis=1)
            right = jnp.concatenate([memory[b, h], memory[b + 1, h]], axis=0).astype(BF16)
            carried = carried + jnp.dot(left, right, preferred_element_type=F32)
        head_out = (forget * carried + fresh) / denom
        normed = head_out * lax.rsqrt(jnp.mean(head_out * head_out, axis=1, keepdims=True) + EPSILON)
        gate = jax.nn.sigmoid(outgate[:, h * VD : (h + 1) * VD])
        mixed = (normed * gain[h : h + 1, :] * gate).astype(BF16)
        heads[:, :, h * VD : (h + 1) * VD] = jnp.broadcast_to(mixed[None], (heads.shape[0], seqs, VD))


def state_step(recv, forget_bias, memory, normalizer, stabilizer, head_gain, model_width, total_heads):
    blocks = recv.shape[0]
    seqs, local = memory.shape[:2]

    def kernel(*refs):
        state_kernel(*refs, model_width=model_width, total_heads=total_heads)

    return pl.pallas_call(
        kernel,
        out_shape=(
            jax.ShapeDtypeStruct((blocks, seqs, local * VD), BF16),
            jax.ShapeDtypeStruct((seqs, local, QK), F32),
            jax.ShapeDtypeStruct((local, seqs), F32),
            jax.ShapeDtypeStruct((seqs, local, LANES), F32),
            jax.ShapeDtypeStruct((seqs, local, QK), F32),
            jax.ShapeDtypeStruct((seqs, local, VD), F32),
        ),
        in_specs=[spec(VMEM)] * 6,
        out_specs=[spec(VMEM)] * 6,
        compiler_params=pltpu.CompilerParams(vmem_limit_bytes=16 << 20),
        name="state",
    )(recv, forget_bias[None], memory, normalizer, stabilizer.T, head_gain)


def split_job(gain, wg, wu, gate_sets, up_sets):
    half = LANES // 2
    low = lax.broadcasted_iota(jnp.int32, (wg.shape[0], LANES), 1) < half
    for src, dst in ((wg, gate_sets), (wu, up_sets)):
        for at in range(0, src.shape[1], 2 * LANES):
            one, two = (
                (src[:, lo : lo + LANES].astype(F32) * gain[:, lo : lo + LANES]).astype(BF16)
                for lo in (at, at + LANES)
            )
            first = jnp.where(low, one, pltpu.roll(two, half, 1))
            second = jnp.where(low, pltpu.roll(one, half, 1), two)
            dst[0, :, at // 2 : at // 2 + LANES] = first
            dst[1, :, at // 2 : at // 2 + LANES] = second


def partial_sums(rows_ref, gate_sets, up_sets, side):
    blocks, half, rows = rows_ref.shape
    square = jnp.zeros((half, rows), F32)
    for j in range(blocks):
        value = rows_ref[j].astype(F32)
        square = square + value * value
    flat = rows_ref[...].reshape(blocks * half, rows)
    gate = jnp.dot(gate_sets[side], flat, preferred_element_type=F32)
    up = jnp.dot(up_sets[side], flat, preferred_element_type=F32)
    return gate, up, square


def near_job(wd, mine, gate_sets, up_sets, turned, gate, up, square):
    turn_job(wd, turned)
    gate[...], up[...], square[...] = partial_sums(mine, gate_sets, up_sets, lax.axis_index("tp"))


def turn_job(wd, turned):
    cols = turned.shape[1]
    for j in range(turned.shape[0]):
        turned[j] = wd[:, j * cols : (j + 1) * cols].T


def down_half(turned, hidden, out, side):
    blocks, half, rows = out.shape
    at = pl.multiple_of(side * half, half)
    for j in range(blocks):
        part = jnp.dot(turned[j, pl.ds(at, half), :], hidden, preferred_element_type=F32)
        out[j] = part.astype(BF16)


def keep_job(turned, hidden, keep):
    down_half(turned, hidden[...], keep, lax.axis_index("tp"))


def memory_kernel(*refs, first, count, kept, job, reads):
    memory, forget, key, value = refs[:4]
    small = refs[4 : 4 + kept]
    fresh, sems = refs[-2:]
    made = len(refs) - 2 - reads[1]
    outs = refs[made - 1 - kept : made]
    target, small_out = outs[0], outs[1:]
    seqs = memory.shape[0]
    writes = []

    def send(src, dst):
        write = pltpu.make_async_copy(src, dst, sems.at[len(writes)])
        write.start()
        writes.append(write)

    for src, dst in zip(small, small_out):
        send(src, dst)
    key_cols = {}
    for n in range(count):
        h, b = divmod(first + n, seqs)
        if h not in key_cols:
            key_cols[h] = key[:, h, :].T
        decay = forget[b : b + 1, h, :1]
        fresh[n] = decay * memory[b, h] + key_cols[h][:, b : b + 1] * value[b : b + 1, h, :]
        send(fresh.at[n], target.at[b, h])
    job(*refs[4 + kept : 4 + kept + reads[0]], *refs[made:-2])
    for write in writes:
        write.wait()


def memory_step(memory, forget, key, value, first, count, job, needs, makes, partial=None, small=()):
    def kernel(*refs):
        memory_kernel(
            *refs, first=first, count=count, kept=len(small), job=job, reads=(len(needs), len(makes))
        )

    near = [memory, forget, key, value, *small, *needs]
    extra = [] if partial is None else stay(partial)
    outs = [HBM(memory.shape, F32)] + [HBM(a.shape, F32) for a in small]
    kinds = [spec(HBM)] * len(outs) + [spec(VMEM)] * len(makes)
    outs += [jax.ShapeDtypeStruct(shape, kind) for shape, kind in makes]
    return pl.pallas_call(
        kernel,
        out_shape=outs,
        in_specs=[spec(VMEM)] * len(near) + [spec(HBM)] * len(extra),
        out_specs=kinds,
        input_output_aliases={len(near): 0} if extra else {},
        scratch_shapes=[
            pltpu.VMEM((count,) + memory.shape[2:], F32),
            pltpu.SemaphoreType.DMA((count + len(small),)),
        ],
        compiler_params=pltpu.CompilerParams(vmem_limit_bytes=8 << 20),
        cost_estimate=pl.CostEstimate(flops=0, bytes_accessed=0, transcendentals=0),
        name="memory",
    )(*near, *extra)


def mixer_kernel(other, after, near_gate, near_up, near_square, gate_sets, up_sets, turned, give, hidden):
    blocks, half, _ = other.shape
    tp = lax.axis_index("tp")
    gate, up, square = partial_sums(other, gate_sets, up_sets, 1 - tp)
    square = jnp.sum(square + near_square[...], axis=0, keepdims=True)
    inverse = lax.rsqrt(square / (2 * blocks * half) + EPSILON)
    gate = (gate + near_gate[...]) * inverse
    up = (up + near_up[...]) * inverse
    value = (jax.nn.silu(gate) * up).astype(BF16)
    hidden[...] = value
    down_half(turned, value, give, 1 - tp)


def mixer(other, after, *near):
    blocks, half, rows = other.shape
    return pl.pallas_call(
        mixer_kernel,
        out_shape=(
            jax.ShapeDtypeStruct((blocks, half, rows), BF16),
            jax.ShapeDtypeStruct(near[0].shape, BF16),
        ),
        in_specs=[spec(VMEM), spec(HBM)] + [spec(VMEM)] * len(near),
        out_specs=[spec(VMEM)] * 2,
        compiler_params=pltpu.CompilerParams(vmem_limit_bytes=8 << 20),
        name="mixer",
    )(other, *stay(after), *near)


def halves(turned):
    half = turned.shape[0] // 2
    low = lax.axis_index("tp") == 0
    first, second = turned[:half], turned[half:]
    return jnp.where(low, first, second), jnp.where(low, second, first)


def branch_kernel(heads, w_out, keep, give):
    rows = heads[...].reshape(heads.shape[0] * heads.shape[1], w_out.shape[0])
    mine, other = halves(jnp.dot(rows, w_out[...], preferred_element_type=F32).T)
    keep[...] = mine.astype(BF16)
    give[...] = other.astype(BF16)


def branch_step(heads, w_out, *early):
    result = jax.ShapeDtypeStruct((w_out.shape[1] // 2, heads.shape[0] * heads.shape[1]), BF16)
    return pl.pallas_call(
        branch_kernel,
        out_shape=(result, result),
        in_specs=[spec(VMEM)] * (2 + len(early)),
        out_specs=[spec(VMEM)] * 2,
        compiler_params=pltpu.CompilerParams(vmem_limit_bytes=4 << 20),
        name="branch",
    )(heads, w_out, *early)


def pair_kernel(keep, got, after, out):
    out[...] = (keep[...].astype(F32) + got[...].astype(F32)).astype(BF16)


def pair_step(keep, got, after):
    return pl.pallas_call(
        pair_kernel,
        out_shape=jax.ShapeDtypeStruct(keep.shape, BF16),
        in_specs=[spec(VMEM)] * 2 + [spec(HBM)],
        out_specs=spec(VMEM),
        compiler_params=pltpu.CompilerParams(vmem_limit_bytes=4 << 20),
        name="pair",
    )(keep, got, *stay(after))


def residual_kernel(tokens, keep, got, after, spread, own):
    mine, _ = halves(tokens[...].astype(F32).T)
    rounded = (mine + (keep[...].astype(F32) + got[...].astype(F32))).astype(BF16)
    own[...] = rounded
    spread[...] = jnp.broadcast_to(rounded[None], spread.shape)


def residual_step(tokens, keep, got, after, blocks):
    return pl.pallas_call(
        residual_kernel,
        out_shape=(
            jax.ShapeDtypeStruct((blocks,) + keep.shape, BF16),
            jax.ShapeDtypeStruct(keep.shape, BF16),
        ),
        in_specs=[spec(VMEM)] * 3 + [spec(HBM)],
        out_specs=[spec(VMEM)] * 2,
        compiler_params=pltpu.CompilerParams(vmem_limit_bytes=4 << 20),
        name="residual",
    )(tokens, keep, got, *stay(after))


def finish_kernel(recv, own, out):
    out[...] = (jnp.sum(recv[...].astype(F32), axis=0) + own[...].astype(F32)).astype(BF16)


def finish(recv, own):
    return pl.pallas_call(
        finish_kernel,
        out_shape=jax.ShapeDtypeStruct(own.shape, BF16),
        in_specs=[spec(VMEM)] * 2,
        out_specs=spec(VMEM),
        compiler_params=pltpu.CompilerParams(vmem_limit_bytes=4 << 20),
        name="finish",
    )(recv, own)


def other_core(value):
    return lax.ppermute(value, "tp", [(0, 1), (1, 0)])


def exchanged(blocks):
    return lax.all_to_all(blocks, "kv", 0, 0, tiled=True)


def body(
    tokens,
    mix_gain,
    w_query,
    w_key,
    w_value,
    w_outgate,
    w_gates,
    forget_bias,
    memory,
    normalizer,
    stabilizer,
    head_gain,
    w_out,
    mlp_gain,
    w_gate,
    w_up,
    w_down,
):
    devices = lax.axis_size("kv")
    rows, block_cols = tokens.shape
    send = project(tokens, mix_gain, w_query, w_key, w_value, w_outgate, w_gates, devices)
    heads, new_normalizer, new_stabilizer, forget, key, value_heads = state_step(
        exchanged(send),
        forget_bias,
        memory,
        normalizer,
        stabilizer,
        head_gain,
        block_cols * devices,
        w_gates.shape[1] // 2,
    )
    def behind(value):
        return lax.optimization_barrier((forget, key, value_heads, value))[:3]

    units = memory.shape[0] * memory.shape[1]
    early, share = 7 * units // 32, 11 * units // 32
    wg, wu = w_gate.T, w_up.T
    keep, give = branch_step(exchanged(heads), w_out)
    sets = (2, wg.shape[0], wg.shape[1] // 2)
    part, new_normalizer, new_stabilizer, gate_sets, up_sets = memory_step(
        memory, *behind(give), 0, early, split_job, (mlp_gain[None], wg, wu),
        ((sets, BF16), (sets, BF16)), small=(new_normalizer, new_stabilizer),
    )
    spread, own = residual_step(tokens, keep, other_core(give), part, devices)
    mine = exchanged(spread)
    hidden_shape = (wg.shape[0], rows)
    part, turned, *near = memory_step(
        memory, *behind(mine), early, share, near_job, (w_down, mine, gate_sets, up_sets),
        (((devices, block_cols, w_down.shape[0]), BF16), (hidden_shape, F32), (hidden_shape, F32), (own.shape, F32)),
        part,
    )
    give, hidden = mixer(other_core(mine), part, *near, gate_sets, up_sets, turned)
    new_memory, keep = memory_step(
        memory, *behind(give), early + share, units - early - share, keep_job, (turned, hidden),
        ((give.shape, BF16),), part,
    )
    pair = pair_step(keep, other_core(give), new_memory)
    mixed_out = finish(exchanged(pair), own).T
    return (mixed_out, new_memory, new_normalizer, new_stabilizer.T)


def solution(mesh):
    in_specs = (
        P("dp", "kv"),
        P("kv"),
        P("kv", "tp"),
        P("kv", "tp"),
        P("kv", "tp"),
        P("kv", "tp"),
        P(),
        P("tp"),
        P(("dp", "kv"), "tp", None, None),
        P(("dp", "kv"), "tp", None),
        P(("dp", "kv"), "tp"),
        P("tp", None),
        P("tp", "kv"),
        P(),
        P(None, ("kv", "tp")),
        P(None, ("kv", "tp")),
        P(("kv", "tp"), None),
    )
    out_specs = (
        P("dp", ("kv", "tp")),
        P(("dp", "kv"), "tp", None, None),
        P(("dp", "kv"), "tp", None),
        P(("dp", "kv"), "tp"),
    )
    return jax.shard_map(body, mesh=mesh, in_specs=in_specs, out_specs=out_specs, check_vma=False)
```
